128 devices in a mesh: sp: 32 (over z, y, core), tp: 4 (over x).
Axes of the slice: x: 4, y: 4, z: 4, core: 2. Of those that a mesh axis runs over, the one named last changes fastest.
Arguments:
- stream: bfloat16 [16384, 2048], P(('sp', 'tp')), may hold values from -6 to 6
- conv_in_a: bfloat16 [16384, 1024], P('sp', 'tp'), may hold values from -6 to 6
- conv_in_b: bfloat16 [16384, 1024], P('sp', 'tp'), may hold values from -6 to 6
- gate_in_a: bfloat16 [16384, 1024], P('sp', 'tp'), may hold values from -6 to 6
- gate_in_b: bfloat16 [16384, 1024], P('sp', 'tp'), may hold values from -6 to 6
- conv_w_a: bfloat16 [4, 1024], P(None, 'tp'), may hold values from -3 to 3
- conv_w_b: bfloat16 [4, 1024], P(None, 'tp'), may hold values from -3 to 3
- rec_gate_a: bfloat16 [16, 64, 64], P('tp'), may hold values from -0.75 to 0.75
- inp_gate_a: bfloat16 [16, 64, 64], P('tp'), may hold values from -0.75 to 0.75
- rec_gate_b: bfloat16 [8, 128, 128], P('tp'), may hold values from -0.5 to 0.5
- inp_gate_b: bfloat16 [8, 128, 128], P('tp'), may hold values from -0.5 to 0.5
- decay_a: float32 [1024], P('tp'), may hold values from 3 to 20
- decay_b: float32 [1024], P('tp'), may hold values from 3 to 20
- decay_increments: float32 [16384], P('sp'), may hold values from -0.7 to 0
- out_w_a: bfloat16 [1024, 2048], P('tp'), may hold values from -0.5 to 0.5
- out_w_b: bfloat16 [1024, 2048], P('tp'), may hold values from -0.5 to 0.5
- norm_gain: bfloat16 [2048], replicated, may hold values from 0.099609375 to 1.8984375
- expert_ids: int32 [16384, 2], P(('sp', 'tp')), may hold values from 0 to 127, as said below
- group_prob: float32 [16384], P(('sp', 'tp')), may hold values from 0.3 to 1
- pick_gap: float32 [16384], P(('sp', 'tp')), may hold values from -6 to 6
- w_gate: bfloat16 [128, 2048, 1024], P(('sp', 'tp')), may hold values from -0.125 to 0.125
- w_up: bfloat16 [128, 2048, 1024], P(('sp', 'tp')), may hold values from -0.125 to 0.125
- w_down: bfloat16 [128, 1024, 2048], P(('sp', 'tp')), may hold values from -0.5 to 0.5
Outputs:
- result: bfloat16 [16384, 2048], P(('sp', 'tp'))
The draws below stay inside these ranges and needn't reach their ends.
Inputs may be any that keep to these rules, and one draw needn't show every extreme that they name: `expert_ids`: each row names two different experts of one group: both lie in g * 32 to g * 32 + 31 for some g. In each aligned block of 128 rows no expert is named more than 4 times, and in every block some expert is named exactly 4 times.
All inputs are finite; a program needn't handle non-finite values.
Results may differ from the reference program's by a relative error of at most 0.015.
Values may be sent and summed in bfloat16 or wider, within the bound.
A program may use at most 128 MiB of HBM per device.

```python
import math
import jax
import jax.numpy as jnp
from jax import lax

D = 2048
HEADS_A = 16
DIM_A = 64
HEADS_B = 8
DIM_B = 128
WIDTH_A = 1024
WIDTH_B = 1024
D_LRU = 2048
CONV_TAPS = 4
FFN_HIDDEN = 1024
EXPERTS = 128
GROUPS = 4
SEQUENCE_TOKENS = 16384
ROWS = 128
CAP = 4


def decay_levels(base_key, head_count, head_dim):
    random_subkeys = jax.random.split(base_key, 4)
    slow_share = 0.5
    is_slow = jax.random.uniform(random_subkeys[0], (head_count,), jnp.float32) < slow_share
    slow_rate = jnp.exp(jax.random.uniform(random_subkeys[1], (head_count,), jnp.float32, math.log(0.05 / SEQUENCE_TOKENS), math.log(0.5 / SEQUENCE_TOKENS)))
    fast_rate = jnp.exp(jax.random.uniform(random_subkeys[2], (head_count,), jnp.float32, math.log(0.004), math.log(0.03)))
    head_rate = jnp.where(is_slow, slow_rate, fast_rate)
    spread = jnp.exp(jax.random.uniform(random_subkeys[3], (head_count * head_dim,), jnp.float32, -0.35, 0.35))
    channel_rate = jnp.repeat(head_rate, head_dim) * spread
    return (-jnp.log(jnp.expm1(channel_rate))).astype(jnp.float32)


def draw_decay_a(key, part):
    return decay_levels(jax.random.fold_in(key, 11), HEADS_A, DIM_A)


def draw_decay_b(key, part):
    return decay_levels(jax.random.fold_in(key, 12), HEADS_B, DIM_B)


def draw_decay_increments(key, part):
    random_subkeys = jax.random.split(jax.random.fold_in(key, 13), 2)
    surge_count = 8
    surge_position = jax.random.randint(random_subkeys[0], (surge_count,), 0, SEQUENCE_TOKENS)
    surge_depth = jnp.log(jax.random.uniform(random_subkeys[1], (surge_count,), jnp.float32, 0.5, 0.8))
    return jnp.zeros((SEQUENCE_TOKENS,), jnp.float32).at[surge_position].set(surge_depth)


def group_order(block_key):
    return jax.random.permutation(block_key, GROUPS)


def row_order(block_key):
    return jax.random.permutation(block_key, ROWS)


def draw_expert_ids(key, part):
    random_subkeys = jax.random.split(jax.random.fold_in(key, 14), 4)
    block_total = SEQUENCE_TOKENS // ROWS
    group_width = EXPERTS // GROUPS
    orders = jax.vmap(group_order)(jax.random.split(random_subkeys[0], block_total))
    offsets = jax.random.randint(random_subkeys[1], (block_total, 3), 0, group_width)
    partner_steps = jax.random.randint(random_subkeys[3], (block_total, 3), 1, group_width)
    position = jnp.arange(ROWS, dtype=jnp.int32)
    half_rows = ROWS // 2
    quarter_rows = ROWS // 4
    slot_rank = (position >= half_rows).astype(jnp.int32) + (position >= half_rows + quarter_rows).astype(jnp.int32)
    starts = jnp.where(slot_rank == 0, 0, jnp.where(slot_rank == 1, half_rows, half_rows + quarter_rows))
    within = position - starts
    rank_rows = jnp.broadcast_to(slot_rank[None, :], (block_total, ROWS))
    group_ids = jnp.take_along_axis(orders, rank_rows, axis=1)
    offset_rows = jnp.take_along_axis(offsets, rank_rows, axis=1)
    step_rows = jnp.take_along_axis(partner_steps, rank_rows, axis=1)
    first_pick = (offset_rows + within[None, :]) % group_width
    second_pick = (first_pick + step_rows) % group_width
    pairs = jnp.stack([group_ids * group_width + first_pick, group_ids * group_width + second_pick], axis=-1)
    shuffles = jax.vmap(row_order)(jax.random.split(random_subkeys[2], block_total))
    pairs = jnp.take_along_axis(pairs, shuffles[:, :, None], axis=1)
    return pairs.reshape(SEQUENCE_TOKENS, 2).astype(jnp.int32)


def block_scale(key, shape, pieces, smallest, largest):
    factor_of = 1.0
    for dim, parts in pieces:
        draws = jax.random.uniform(jax.random.fold_in(jax.random.fold_in(key, 6), dim), (parts,), jnp.float32, smallest / len(pieces), largest / len(pieces))
        factor_of = factor_of * jnp.repeat(jnp.exp(draws), shape[dim] // parts).reshape((-1,) + (1,) * (len(shape) - 1 - dim))
    return factor_of


def noise(key, dims, scale, most, cuts=(), kind=jnp.bfloat16):
    drawn = scale * jax.random.normal(key, dims, jnp.float32)
    if cuts:
        drawn = drawn * block_scale(key, dims, cuts, -0.22, 0.18)
    return jnp.clip(drawn, -most, most).astype(kind)


def setup_inputs(seed: int = 0) -> dict:
    key_of = jax.random.split(jax.random.key(seed), 24)
    return {
        "stream": noise(key_of[0], (SEQUENCE_TOKENS, D), 1.0, 6.0, ((0, 128),)),
        "conv_in_a": noise(key_of[1], (SEQUENCE_TOKENS, WIDTH_A), 1.0, 6.0, ((0, 32), (1, 4))),
        "conv_in_b": noise(key_of[2], (SEQUENCE_TOKENS, WIDTH_B), 1.0, 6.0, ((0, 32), (1, 4))),
        "gate_in_a": noise(key_of[3], (SEQUENCE_TOKENS, WIDTH_A), 1.0, 6.0, ((0, 32), (1, 4))),
        "gate_in_b": noise(key_of[4], (SEQUENCE_TOKENS, WIDTH_B), 1.0, 6.0, ((0, 32), (1, 4))),
        "conv_w_a": noise(key_of[5], (CONV_TAPS, WIDTH_A), CONV_TAPS ** -0.5, 3.0, ((1, 4),)),
        "conv_w_b": noise(key_of[6], (CONV_TAPS, WIDTH_B), CONV_TAPS ** -0.5, 3.0, ((1, 4),)),
        "rec_gate_a": noise(key_of[7], (HEADS_A, DIM_A, DIM_A), DIM_A ** -0.5, 0.75, ((0, 4),)),
        "inp_gate_a": noise(key_of[8], (HEADS_A, DIM_A, DIM_A), DIM_A ** -0.5, 0.75, ((0, 4),)),
        "rec_gate_b": noise(key_of[9], (HEADS_B, DIM_B, DIM_B), DIM_B ** -0.5, 0.5, ((0, 4),)),
        "inp_gate_b": noise(key_of[10], (HEADS_B, DIM_B, DIM_B), DIM_B ** -0.5, 0.5, ((0, 4),)),
        "decay_a": draw_decay_a(jax.random.fold_in(key_of[23], 71), 0),
        "decay_b": draw_decay_b(jax.random.fold_in(key_of[23], 71), 0),
        "decay_increments": draw_decay_increments(jax.random.fold_in(key_of[23], 71), 0),
        "out_w_a": noise(key_of[14], (WIDTH_A, D), (D_LRU // 16) ** -0.5, 0.5, ((0, 4),)),
        "out_w_b": noise(key_of[15], (WIDTH_B, D), (D_LRU // 16) ** -0.5, 0.5, ((0, 4),)),
        "norm_gain": jnp.clip(1.0 + 0.18 * jax.random.normal(key_of[16], (D,), jnp.float32), 0.099609375, 1.8984375).astype(jnp.bfloat16),
        "expert_ids": draw_expert_ids(jax.random.fold_in(key_of[23], 71), 0),
        "group_prob": jnp.clip(0.3 + 0.7 * jax.random.uniform(key_of[18], (SEQUENCE_TOKENS,), jnp.float32) ** block_scale(key_of[18], (SEQUENCE_TOKENS,), ((0, 128),), -0.2, 0.2), 0.3, 1.0),
        "pick_gap": noise(key_of[19], (SEQUENCE_TOKENS,), 1.5, 6.0, ((0, 128),), jnp.float32),
        "w_gate": noise(key_of[20], (EXPERTS, D, FFN_HIDDEN), D ** -0.5, 0.125, ((0, 128),)),
        "w_up": noise(key_of[21], (EXPERTS, D, FFN_HIDDEN), D ** -0.5, 0.125, ((0, 128),)),
        "w_down": noise(key_of[22], (EXPERTS, FFN_HIDDEN, D), (FFN_HIDDEN // 8) ** -0.5, 0.5, ((0, 128),)),
    }


EPSILON = 1e-06
GATE_SCALE = 8.0

def causal_taps(source, weights):
    length = source.shape[0]
    tap_count = weights.shape[0]
    padded = jnp.pad(source.astype(jnp.float32), ((tap_count - 1, 0), (0, 0)))
    total = jnp.zeros(source.shape, jnp.float32)
    for offset in range(tap_count):
        total = total + weights[offset].astype(jnp.float32)[None, :] * padded[offset:offset + length]
    return total.astype(jnp.bfloat16)

def recurrence_inputs(conv_out, rec_gate, inp_gate, decay, jump_log):
    length = conv_out.shape[0]
    head_count = rec_gate.shape[0]
    head_dim = rec_gate.shape[1]
    blocks = conv_out.astype(jnp.float32).reshape(length, head_count, head_dim)
    recur = jax.nn.sigmoid(jnp.einsum('thi,hij->thj', blocks, rec_gate.astype(jnp.float32)).reshape(length, -1))
    admit = jax.nn.sigmoid(jnp.einsum('thi,hij->thj', blocks, inp_gate.astype(jnp.float32)).reshape(length, -1))
    log_decay = -GATE_SCALE * recur * jax.nn.softplus(-decay)[None, :] + jump_log[:, None]
    drive = jnp.sqrt(-jnp.expm1(2.0 * log_decay)) * admit * conv_out.astype(jnp.float32)
    return (jnp.exp(log_decay), drive)

def link_states(earlier, later):
    return (earlier[0] * later[0], later[0] * earlier[1] + later[1])

def block_slots(block_ids):
    onehot = (block_ids[:, None] == jnp.arange(EXPERTS, dtype=jnp.int32)[None, :]).astype(jnp.int32)
    return (lax.optimization_barrier(jnp.sum(jnp.cumsum(onehot, axis=0) * onehot, axis=1)) - 1).astype(jnp.int32)

def route_experts(normed, expert_ids, w_gate, w_up, w_down):
    block_total = SEQUENCE_TOKENS // ROWS
    flat_ids = expert_ids.reshape(block_total, 2 * ROWS).astype(jnp.int32)
    slots = lax.map(block_slots, flat_ids)
    block_index = jnp.broadcast_to(jnp.arange(block_total, dtype=jnp.int32)[:, None], flat_ids.shape)
    token_index = (block_index * ROWS + jnp.arange(2 * ROWS, dtype=jnp.int32)[None, :] // 2).astype(jnp.int32)
    table = jnp.full((EXPERTS, block_total, CAP), SEQUENCE_TOKENS, jnp.int32).at[flat_ids, block_index, slots].set(token_index)
    padded_rows = jnp.concatenate([normed, jnp.zeros((1, D), jnp.bfloat16)], axis=0)

    def one_expert(operands):
        gate_weight, up_weight, down_weight, index_rows = operands
        rows_in = padded_rows[index_rows.reshape(-1)]
        gate_part = jnp.dot(rows_in, gate_weight, preferred_element_type=jnp.float32)
        up_part = jnp.dot(rows_in, up_weight, preferred_element_type=jnp.float32)
        inner = (jax.nn.silu(gate_part) * up_part).astype(jnp.bfloat16)
        return jnp.dot(inner, down_weight, preferred_element_type=jnp.float32).astype(jnp.bfloat16)
    outputs = lax.map(one_expert, (w_gate, w_up, w_down, table))
    place = (flat_ids * (block_total * CAP) + block_index * CAP + slots).reshape(-1).astype(jnp.int32)
    picked = outputs.reshape(-1, D)[place]
    return picked.reshape(SEQUENCE_TOKENS, 2, D)

def reference(stream, conv_in_a, conv_in_b, gate_in_a, gate_in_b, conv_w_a, conv_w_b, rec_gate_a, inp_gate_a, rec_gate_b, inp_gate_b, decay_a, decay_b, decay_increments, out_w_a, out_w_b, norm_gain, expert_ids, group_prob, pick_gap, w_gate, w_up, w_down):
    conv_a = causal_taps(conv_in_a, conv_w_a)
    conv_b = causal_taps(conv_in_b, conv_w_b)
    factor_a, drive_a = recurrence_inputs(conv_a, rec_gate_a, inp_gate_a, decay_a, decay_increments)
    factor_b, drive_b = recurrence_inputs(conv_b, rec_gate_b, inp_gate_b, decay_b, decay_increments)
    states_a = lax.associative_scan(link_states, (factor_a, drive_a), axis=0)[1]
    states_b = lax.associative_scan(link_states, (factor_b, drive_b), axis=0)[1]
    hidden_a = (states_a * jax.nn.gelu(gate_in_a.astype(jnp.float32))).astype(jnp.bfloat16)
    hidden_b = (states_b * jax.nn.gelu(gate_in_b.astype(jnp.float32))).astype(jnp.bfloat16)
    mixed_rows = jnp.dot(hidden_a, out_w_a, preferred_element_type=jnp.float32) + jnp.dot(hidden_b, out_w_b, preferred_element_type=jnp.float32)
    middle = (stream.astype(jnp.float32) + mixed_rows).astype(jnp.bfloat16)
    middle_f = middle.astype(jnp.float32)
    scale_rows = lax.rsqrt(lax.optimization_barrier(jnp.mean(middle_f * middle_f, axis=-1, keepdims=True)) + EPSILON)
    normed = (middle_f * scale_rows * norm_gain.astype(jnp.float32)[None, :]).astype(jnp.bfloat16)
    picked = route_experts(normed, expert_ids, w_gate, w_up, w_down)
    first_weight = group_prob * jax.nn.sigmoid(pick_gap)
    second_weight = group_prob * jax.nn.sigmoid(-pick_gap)
    total = middle_f + first_weight[:, None] * picked[:, 0].astype(jnp.float32) + second_weight[:, None] * picked[:, 1].astype(jnp.float32)
    return total.astype(jnp.bfloat16)
```

```python
import jax
import jax.numpy as jnp
from jax import lax
from jax.experimental import pallas as pl
from jax.experimental.pallas import tpu as pltpu
from jax.sharding import PartitionSpec as P

EPSILON = 1e-06
GATE_SCALE = 8.0
F32 = jnp.float32
BF16 = jnp.bfloat16
MESH = pl.DeviceIdType.MESH
ROWS = 128
LEN = 512
CH = 512
D = 2048
Q = 512
HID = 1024
SPN = 32


def dot(a, b):
    return jnp.dot(a, b, preferred_element_type=F32)


def iota(shape, dim):
    return lax.broadcasted_iota(jnp.int32, shape, dim)


def one_minus_exp(u):
    series = u * (
        1.0
        - u
        * (
            0.5
            - u
            * (
                1.0 / 6
                - u * (1.0 / 24 - u * (1.0 / 120 - u * (1.0 / 720 - u * (1.0 / 5040))))
            )
        )
    )
    return jnp.where(u < 0.25, series, 1.0 - jnp.exp(-u))


def softplus_neg(d):
    y = jnp.exp(-jnp.abs(d))
    w = 1.0 + y
    near = w - 1.0
    log1p = jnp.where(near == 0.0, y, jnp.log(w) * (y / jnp.where(near == 0.0, 1.0, near)))
    return jnp.maximum(-d, 0.0) + log1p


def shift_of(k):
    c, j = k // 32, k % 32
    dc, dx, dy = j % 2, (j // 2) % 4, (j // 8) % 4
    dz = (c + 8 - dx - dy) % 4
    return dz, dy, dc, dx


def kernel(
    stream,
    cia,
    cib,
    gia,
    gib,
    cwa,
    cwb,
    rga,
    iga,
    rgb,
    igb,
    da,
    db,
    inc,
    owa,
    owb,
    gain,
    ids,
    gp,
    pg,
    wg_hbm,
    wu_hbm,
    wd_hbm,
    out,
    wg,
    wu,
    wd,
    ow,
    xs,
    wb,
    incb,
    a8,
    h8,
    gl,
    hid,
    halo,
    stat,
    carry_in,
    psend,
    rd2,
    prec,
    p0,
    nq,
    mp,
    gm,
    sendb,
    recvb,
    replyb,
    retb,
    xb,
    inner,
    yb,
    acc,
    keys,
    lsem,
    hsem,
    csem,
    psem,
    dsem,
    rsem,
):
    sp = lax.axis_index("sp")
    x = lax.axis_index("tp")
    z, y, core = sp // 8, (sp // 2) % 4, sp % 2

    def device(dz, dy, dc, dx):
        nz, ny, nc = (z + dz) % 4, (y + dy) % 4, (core + dc) % 2
        return {"sp": (nz * 4 + ny) * 2 + nc, "tp": (x + dx) % 4}

    def away(k):
        dz, dy, dc, dx = shift_of(k)
        return device(dz, dy, dc, dx)

    def back(k):
        dz, dy, dc, dx = shift_of(k)
        return device(4 - dz, 4 - dy, 2 - dc, 4 - dx)

    barrier = pltpu.get_barrier_semaphore()

    def greet(k, carry):
        pl.semaphore_signal(barrier, inc=1, device_id=away(k), device_id_type=MESH)
        return carry

    lax.fori_loop(1, 128, greet, 0)

    loads = [
        pltpu.make_async_copy(owa, ow.at[pl.ds(0, 256)], lsem.at[0]),
        pltpu.make_async_copy(owb, ow.at[pl.ds(256, 256)], lsem.at[1]),
        pltpu.make_async_copy(wg_hbm.at[0], wg, lsem.at[2]),
        pltpu.make_async_copy(wu_hbm.at[0], wu, lsem.at[3]),
        pltpu.make_async_copy(wd_hbm.at[0], wd, lsem.at[4]),
    ]
    for load in loads:
        load.start()

    for n, (a_ref, b_ref) in enumerate(((rga, rgb), (iga, igb))):
        for h in range(4):
            place = (iota((64, 256), 1) == iota((64, 256), 0) + 64 * h).astype(BF16)
            wb[n, 64 * h : 64 * h + 64, :] = dot(a_ref[h], place).astype(BF16)
        wb[2 + n] = jnp.zeros((256, 256), BF16)
        for h in range(2):
            wb[2 + n, 128 * h : 128 * h + 128, 128 * h : 128 * h + 128] = b_ref[h]

    for n in range(4):
        row = jnp.broadcast_to(inc[:, 128 * n : 128 * n + 128], (128, 128))
        incb[128 * n : 128 * n + 128, :] = row.T

    xs[0:8, :] = jnp.zeros((8, CH), F32)
    xs[8 : 8 + LEN, 0:256] = cia[...].astype(F32)
    xs[8 : 8 + LEN, 256:512] = cib[...].astype(F32)

    plus = softplus_neg(jnp.concatenate([da[...], db[...]], axis=1)) * GATE_SCALE

    def chunk(step):
        r0 = pl.multiple_of(step * 64, 64)
        jump = incb[pl.ds(r0, 64), :]
        jump = jnp.concatenate([jump, jump], axis=1)
        for side, taps in enumerate((cwa, cwb)):
            lanes = slice(256 * side, 256 * side + 256)
            window = xs[pl.ds(r0, 72), lanes]
            tap = taps[...].astype(F32)
            total = tap[0:1] * pltpu.roll(window, 3, 0)[8:]
            total = total + tap[1:2] * pltpu.roll(window, 2, 0)[8:]
            total = total + tap[2:3] * pltpu.roll(window, 1, 0)[8:]
            total = total + tap[3:4] * window[8:]
            conv = total.astype(BF16)
            rec = jax.nn.sigmoid(dot(conv, wb[2 * side]))
            admit = jax.nn.sigmoid(dot(conv, wb[2 * side + 1]))
            log = jump - rec * plus[:, lanes]
            gone = one_minus_exp(-2.0 * log)
            root = gone * lax.rsqrt(jnp.maximum(gone, 1e-37))
            h = root * admit * conv.astype(F32)
            a = jnp.exp(log)
            a3, h3 = a.reshape(8, 8, 256), h.reshape(8, 8, 256)
            at = iota((8, 8, 256), 1)
            for s in (1, 2, 4):
                ok = at >= s
                ap = jnp.where(ok, pltpu.roll(a3, s, 1), 1.0)
                hp = jnp.where(ok, pltpu.roll(h3, s, 1), 0.0)
                h3 = h3 + a3 * hp
                a3 = a3 * ap
            a8[pl.ds(r0, 64), lanes] = a3.reshape(64, 256)
            h8[pl.ds(r0, 64), lanes] = h3.reshape(64, 256)

    def later_chunks(step, carry):
        chunk(7 - step)
        return carry

    lax.fori_loop(0, 7, later_chunks, 0)

    e0 = jnp.broadcast_to(ids[:, 0:1].astype(F32), (128, 128))
    e1 = jnp.broadcast_to(ids[:, 1:2].astype(F32), (128, 128))
    e0r, e1r = e0.T, e1.T
    earlier = iota((128, 128), 0) < iota((128, 128), 1)
    for n, er in enumerate((e0r, e1r)):
        hits = jnp.where(earlier & (e0 == er), 1.0, 0.0) + jnp.where(earlier & (e1 == er), 1.0, 0.0)
        rank = jnp.sum(hits, axis=0, keepdims=True).astype(jnp.int32)
        e = er[0:1].astype(jnp.int32)
        ez, ey, ec, ex = e // 32, (e // 8) % 4, (e // 4) % 2, e % 4
        dz, dy, dc, dx = (ez - z + 4) % 4, (ey - y + 4) % 4, (ec - core + 2) % 2, (ex - x + 4) % 4
        key = (((dx + dy + dz) % 4) * 32 + dy * 8 + dx * 2 + dc) * 16 + rank
        keys[n] = jnp.broadcast_to(key.astype(F32), (128, 128))
    first = gp[...] * jax.nn.sigmoid(pg[...])
    second = gp[...] * jax.nn.sigmoid(-pg[...])
    keys[2] = jnp.broadcast_to(first, (128, 128)).T
    keys[3] = jnp.broadcast_to(second, (128, 128)).T

    def pack_matrix(step, carry):
        r0 = pl.multiple_of(step * 128, 128)
        rho = (iota((128, 128), 0) + r0).astype(F32)
        k0, k1 = keys[0], keys[1]
        for q in range(4):
            hit = (rho == k0 + 4.0 * q) | (rho == k1 + 4.0 * q)
            mp[pl.ds(r0, 128), 128 * q : 128 * q + 128] = jnp.where(hit, 1.0, 0.0).astype(BF16)
        return carry

    lax.fori_loop(0, 16, pack_matrix, 0)

    pl.semaphore_wait(barrier, 127)
    nextsp = {"sp": (sp + 1) % SPN, "tp": x}
    halos = [
        pltpu.make_async_remote_copy(
            ref.at[pl.ds(LEN - 16, 16)],
            halo.at[n],
            hsem.at[n],
            hsem.at[2 + n],
            device_id=nextsp,
            device_id_type=MESH,
        )
        for n, ref in enumerate((cia, cib))
    ]
    for copy in halos:
        copy.start()

    keys[0] = keys[0].T
    keys[1] = keys[1].T

    def pick_matrix(step, carry):
        r0 = pl.multiple_of(step * 128, 128)
        c, lane = step // 4, step % 4
        rho = (iota((128, 128), 1) + r0).astype(F32)
        k0, k1, w0, w1 = keys[0], keys[1], keys[2], keys[3]
        for q in range(4):
            val = jnp.where(rho == k0 + 4.0 * q, w0, 0.0) + jnp.where(rho == k1 + 4.0 * q, w1, 0.0)
            gm[step, 128 * q : 128 * q + 128, :] = val.astype(BF16)
        return carry

    lax.fori_loop(0, 16, pick_matrix, 0)

    def gelus(step, carry):
        r0 = pl.multiple_of(step * 64, 64)
        gl[pl.ds(r0, 64), 0:256] = jax.nn.gelu(gia[pl.ds(r0, 64), :].astype(F32))
        gl[pl.ds(r0, 64), 256:512] = jax.nn.gelu(gib[pl.ds(r0, 64), :].astype(F32))
        return carry

    lax.fori_loop(0, 8, gelus, 0)

    for copy in halos:
        copy.wait()
    keep = jnp.where(sp > 0, 1.0, 0.0)
    xs[0:8, 0:256] = halo[0].astype(F32)[8:16] * keep
    xs[0:8, 256:512] = halo[1].astype(F32)[8:16] * keep
    chunk(0)

    def link(step, carry):
        prod, state = carry
        for n in range(8):
            r0 = pl.multiple_of(step * 64, 64) + 8 * n
            a, h = a8[pl.ds(r0, 8), :], h8[pl.ds(r0, 8), :]
            h = h + a * state
            a = a * prod
            a8[pl.ds(r0, 8), :] = a
            h8[pl.ds(r0, 8), :] = h
            prod, state = a[7:8], h[7:8]
        return prod, state

    prod, state = lax.fori_loop(0, 8, link, (jnp.ones((1, CH), F32), jnp.zeros((1, CH), F32)))
    for n in range(4):
        stat[n : n + 1, :] = prod[:, 128 * n : 128 * n + 128]
        stat[4 + n : 5 + n, :] = state[:, 128 * n : 128 * n + 128]

    def tell(k, carry):
        pltpu.make_async_remote_copy(
            stat,
            carry_in.at[k],
            csem.at[0],
            csem.at[1],
            device_id={"sp": (sp + k) % SPN, "tp": x},
            device_id_type=MESH,
        ).start()
        return carry

    lax.fori_loop(1, SPN, tell, 0)
    told = carry_in.at[pl.ds(1, SPN - 1)]
    pltpu.make_async_copy(told, told, csem.at[1]).wait()

    enter = jnp.zeros((4, 128), F32)
    for k in range(SPN - 1, 0, -1):
        enter = jnp.where(k <= sp, carry_in[k, 0:4] * enter + carry_in[k, 4:8], enter)
    enter = jnp.concatenate([enter[n : n + 1] for n in range(4)], axis=1)

    def hiddens(step, carry):
        r0 = pl.multiple_of(step * 64, 64)
        states = h8[pl.ds(r0, 64), :] + a8[pl.ds(r0, 64), :] * enter
        hid[pl.ds(r0, 64), :] = (states * gl[pl.ds(r0, 64), :]).astype(BF16)
        return carry

    lax.fori_loop(0, 8, hiddens, 0)

    loads[0].wait()
    loads[1].wait()

    def rows_for(d):
        return hid[pl.ds(pl.multiple_of(((x + d) % 4) * 128, 128), 128), :]

    def project(d, half, extra=None):
        rows = rows_for(d)
        for n in range(2):
            at = 1024 * half + 512 * n
            part = dot(rows, ow[:, at : at + 512])
            if extra is not None:
                part = part + extra[:, 512 * n : 512 * n + 512].astype(F32)
            psend[2 * d + half - 2, :, 512 * n : 512 * n + 512] = part.astype(BF16)

    def push(d, half, dst, sem, dx):
        copy = pltpu.make_async_remote_copy(
            psend.at[2 * d + half - 2],
            dst,
            psem.at[2 * sem],
            psem.at[2 * sem + 1],
            device_id={"sp": sp, "tp": (x + dx) % 4},
            device_id_type=MESH,
        )
        copy.start()
        return copy

    project(2, 0)
    sums = [push(2, 0, rd2.at[0], 0, 1)]
    project(2, 1)
    sums.append(push(2, 1, rd2.at[1], 1, 3))
    project(1, 1)
    sums.append(push(1, 1, prec.at[1], 2, 1))
    project(3, 0)
    sums.append(push(3, 0, prec.at[2], 3, 3))
    own = rows_for(0)
    for n in range(4):
        p0[:, 512 * n : 512 * n + 512] = dot(own, ow[:, 512 * n : 512 * n + 512])
    sums[0].wait_recv()
    project(1, 0, rd2.at[0])
    sums.append(push(1, 0, prec.at[0], 4, 1))
    sums[1].wait_recv()
    project(3, 1, rd2.at[1])
    sums.append(push(3, 1, prec.at[3], 5, 3))
    for copy in sums[2:]:
        copy.wait_recv()

    gains = gain[...].astype(F32)

    def norms(step, carry):
        r0 = pl.multiple_of(step * 16, 16)
        rows = pl.ds(r0, 16)
        mixed = p0[rows, :]
        left = jnp.concatenate([prec[0, rows, :], prec[1, rows, :]], axis=1).astype(F32)
        right = jnp.concatenate([prec[2, rows, :], prec[3, rows, :]], axis=1).astype(F32)
        middle = (stream[rows, :].astype(F32) + (mixed + left + right)).astype(BF16).astype(F32)
        scale = lax.rsqrt(jnp.mean(middle * middle, axis=-1, keepdims=True) + EPSILON)
        normed = (middle * scale * gains).astype(BF16)
        for q in range(4):
            acc[pl.ds(128 * q + r0, 16), :] = middle[:, 512 * q : 512 * q + 512]
            nq[pl.ds(128 * q + r0, 16), :] = normed[:, 512 * q : 512 * q + 512]
        return carry

    lax.fori_loop(0, 8, norms, 0)

    def tile(k):
        return pl.ds(pl.multiple_of(k * 16, 16), 16)

    def out_copy(k):
        return pltpu.make_async_remote_copy(
            sendb.at[tile(k)],
            recvb.at[tile(k)],
            dsem.at[0],
            dsem.at[1 + k // 32],
            device_id=away(k),
            device_id_type=MESH,
        )

    def home_copy(k):
        return pltpu.make_async_remote_copy(
            replyb.at[tile(k)],
            retb.at[tile(k)],
            rsem.at[0],
            rsem.at[1 + k // 32],
            device_id=back(k),
            device_id_type=MESH,
        )

    def dispatch(c, carry):
        for n in range(4):
            r0 = pl.multiple_of(c * 512, 512) + 128 * n
            sendb[pl.ds(r0, 128), :] = dot(mp[pl.ds(r0, 128), :], nq[...]).astype(BF16)

        def go(k, inside):
            out_copy(k).start()
            return inside

        lax.fori_loop(jnp.maximum(c * 32, 1), c * 32 + 32, go, 0)
        return carry

    lax.fori_loop(0, 4, dispatch, 0)
    recvb[0:16, :] = sendb[0:16, :]

    loads[2].wait()
    loads[3].wait()
    loads[4].wait()

    def wait_class(buf, sem, c):
        @pl.when(c == 0)
        def _():
            part = buf.at[pl.ds(16, 496)]
            pltpu.make_async_copy(part, part, sem.at[1]).wait()

        @pl.when(c > 0)
        def _():
            part = buf.at[pl.ds(pl.multiple_of(c * 512, 512), 512)]
            pltpu.make_async_copy(part, part, sem.at[1 + c]).wait()

    def experts(c, carry):
        wait_class(recvb, dsem, c)
        ra, rb = iota((256, 256), 0), iota((256, 256), 1)
        sort = (rb == ((ra % 64) // 4) * 16 + (ra // 64) * 4 + ra % 4).astype(F32).astype(BF16)
        unsort = (ra == ((rb % 64) // 4) * 16 + (rb // 64) * 4 + rb % 4).astype(F32).astype(BF16)
        for half in range(2):
            r0 = pl.multiple_of(c * 512, 512) + 256 * half
            got = dot(sort, recvb[pl.ds(r0, 256), :]).astype(BF16)
            for q in range(4):
                xb[64 * half : 64 * half + 64, 512 * q : 512 * q + 512] = got[64 * q : 64 * q + 64]
        for n in range(4):
            cols = slice(256 * n, 256 * n + 256)
            gate = dot(xb[...], wg[:, cols])
            up = dot(xb[...], wu[:, cols])
            inner[:, cols] = (jax.nn.silu(gate) * up).astype(BF16)
        for q in range(4):
            down = dot(inner[...], wd[:, 512 * q : 512 * q + 512]).astype(BF16)
            for half in range(2):
                yb[half, 64 * q : 64 * q + 64, :] = down[64 * half : 64 * half + 64]
        for half in range(2):
            r0 = pl.multiple_of(c * 512, 512) + 256 * half
            replyb[pl.ds(r0, 256), :] = dot(unsort, yb[half]).astype(BF16)

        def go(k, inside):
            home_copy(k).start()
            return inside

        lax.fori_loop(jnp.maximum(c * 32, 1), c * 32 + 32, go, 0)
        return carry

    lax.fori_loop(0, 4, experts, 0)
    retb[0:16, :] = replyb[0:16, :]

    def combine(c, carry):
        wait_class(retb, rsem, c)
        for n in range(4):
            rows = slice(128 * n, 128 * n + 128)
            part = acc[rows, :]
            for lane in range(4):
                r0 = pl.multiple_of(c * 512, 512) + 128 * lane
                part = part + dot(gm[4 * c + lane, rows, :], retb[pl.ds(r0, 128), :])
            acc[rows, :] = part
        return carry

    lax.fori_loop(0, 4, combine, 0)
    for q in range(4):
        out[:, 512 * q : 512 * q + 512] = acc[128 * q : 128 * q + 128, :].astype(BF16)

    pltpu.make_async_copy(told, told, csem.at[0]).wait()
    for copy in sums:
        copy.wait_send()
    for buf, sem in ((sendb, dsem), (replyb, rsem)):
        part = buf.at[pl.ds(16, 2032)]
        pltpu.make_async_copy(part, part, sem.at[0]).wait()


def shards(*args):
    (
        stream,
        cia,
        cib,
        gia,
        gib,
        cwa,
        cwb,
        rga,
        iga,
        rgb,
        igb,
        da,
        db,
        inc,
        owa,
        owb,
        gain,
        ids,
        gp,
        pg,
        wg,
        wu,
        wd,
    ) = args
    row = lambda a: a.reshape(1, -1)
    operands = (
        stream,
        cia,
        cib,
        gia,
        gib,
        cwa,
        cwb,
        rga,
        iga,
        rgb,
        igb,
        row(da),
        row(db),
        row(inc),
        owa,
        owb,
        row(gain),
        ids,
        row(gp),
        row(pg),
        wg,
        wu,
        wd,
    )
    vmem = pl.BlockSpec(memory_space=pltpu.VMEM)
    far = pl.BlockSpec(memory_space=pl.ANY)
    specs = [vmem] * len(operands)
    for n in (14, 15, 20, 21, 22):
        specs[n] = far
    V = pltpu.VMEM
    return pl.pallas_call(
        kernel,
        out_shape=jax.ShapeDtypeStruct((ROWS, D), BF16),
        in_specs=specs,
        out_specs=vmem,
        scratch_shapes=[
            V((D, HID), BF16),
            V((D, HID), BF16),
            V((HID, D), BF16),
            V((CH, D), BF16),
            V((LEN + 8, CH), F32),
            V((4, 256, 256), BF16),
            V((LEN, 128), F32),
            V((LEN, CH), F32),
            V((LEN, CH), F32),
            V((LEN, CH), F32),
            V((LEN, CH), BF16),
            V((2, 16, 256), BF16),
            V((8, 128), F32),
            V((SPN, 8, 128), F32),
            V((6, ROWS, 1024), BF16),
            V((2, ROWS, 1024), BF16),
            V((4, ROWS, 1024), BF16),
            V((ROWS, D), F32),
            V((512, Q), BF16),
            V((2048, 512), BF16),
            V((16, 512, 128), BF16),
            V((2048, Q), BF16),
            V((2048, Q), BF16),
            V((2048, Q), BF16),
            V((2048, Q), BF16),
            V((128, D), BF16),
            V((128, HID), BF16),
            V((2, 256, Q), BF16),
            V((512, Q), F32),
            V((4, 128, 128), F32),
            pltpu.SemaphoreType.DMA((5,)),
            pltpu.SemaphoreType.DMA((4,)),
            pltpu.SemaphoreType.DMA((2,)),
            pltpu.SemaphoreType.DMA((12,)),
            pltpu.SemaphoreType.DMA((5,)),
            pltpu.SemaphoreType.DMA((5,)),
        ],
        compiler_params=pltpu.CompilerParams(
            collective_id=0, has_side_effects=True, vmem_limit_bytes=58 * 1024 * 1024
        ),
        name="layer",
    )(*operands)


def solution(mesh):
    placed = (
        P(("sp", "tp"), None),
        P("sp", "tp"),
        P("sp", "tp"),
        P("sp", "tp"),
        P("sp", "tp"),
        P(None, "tp"),
        P(None, "tp"),
        P("tp", None, None),
        P("tp", None, None),
        P("tp", None, None),
        P("tp", None, None),
        P("tp"),
        P("tp"),
        P("sp"),
        P("tp", None),
        P("tp", None),
        P(),
        P(("sp", "tp"), None),
        P(("sp", "tp")),
        P(("sp", "tp")),
        P(("sp", "tp"), None, None),
        P(("sp", "tp"), None, None),
        P(("sp", "tp"), None, None),
    )
    return jax.shard_map(
        shards, mesh=mesh, in_specs=placed, out_specs=P(("sp", "tp"), None), check_vma=False
    )
```

```python
import jax
import jax.numpy as jnp
from jax import lax
from jax.experimental import pallas as pl
from jax.experimental.pallas import tpu as pltpu
from jax.sharding import PartitionSpec as P

EPSILON = 1e-06
GATE_SCALE = 8.0
F32 = jnp.float32
BF16 = jnp.bfloat16
MESH = pl.DeviceIdType.MESH
ROWS = 128
LEN = 512
CH = 512
D = 2048
Q = 512
HID = 1024
SPN = 32


def dot(a, b):
    return jnp.dot(a, b, preferred_element_type=F32)


def iota(shape, dim):
    return lax.broadcasted_iota(jnp.int32, shape, dim)


def one_minus_exp(u):
    series = u * (
        1.0
        - u
        * (
            0.5
            - u
            * (
                1.0 / 6
                - u * (1.0 / 24 - u * (1.0 / 120 - u * (1.0 / 720 - u * (1.0 / 5040))))
            )
        )
    )
    return jnp.where(u < 0.25, series, 1.0 - jnp.exp(-u))


def softplus_neg(d):
    y = jnp.exp(-jnp.abs(d))
    w = 1.0 + y
    near = w - 1.0
    log1p = jnp.where(near == 0.0, y, jnp.log(w) * (y / jnp.where(near == 0.0, 1.0, near)))
    return jnp.maximum(-d, 0.0) + log1p


def kernel(
    stream_far,
    cia_far,
    cib_far,
    gia_far,
    gib_far,
    cwa_far,
    cwb_far,
    rga_far,
    iga_far,
    rgb_far,
    igb_far,
    da_far,
    db_far,
    inc_far,
    owa_far,
    owb_far,
    gain_far,
    ids_far,
    gp_far,
    pg_far,
    wg_far,
    wu_far,
    wd_far,
    out,
    stream,
    cia,
    cib,
    gia,
    gib,
    cwa,
    cwb,
    rga,
    iga,
    rgb,
    igb,
    da,
    db,
    inc,
    gain,
    ids,
    gp,
    pg,
    wg,
    wu,
    wd,
    ow,
    xs,
    wb,
    incb,
    a8,
    h8,
    gl,
    hid,
    halo,
    stat,
    carry_in,
    psend,
    rd2,
    prec,
    p0,
    nq,
    mp,
    gm,
    sendb,
    recvb,
    replyb,
    retb,
    xb,
    inner,
    yb,
    acc,
    keys,
    lsem,
    hsem,
    csem,
    psem,
    dsem,
    rsem,
):
    sp = lax.axis_index("sp")
    x = lax.axis_index("tp")
    z, y, core = sp // 8, (sp // 2) % 4, sp % 2

    xs_at = [lax.rem(x + n, 4) for n in range(4)]
    ys_at = [lax.rem(y + n, 4) * 2 for n in range(4)]
    zs_at = [lax.rem(z + n, 4) * 8 for n in range(4)]
    cores_at = [core, 1 - core]
    yc_at = [[ys_at[n] + cores_at[m] for m in range(2)] for n in range(4)]

    def class_devices(c, sign):
        zc = [lax.rem(z + sign * (c - n) + 16, 4) * 8 for n in range(7)]
        found = []
        for j in range(32):
            dc, dx, dy = j % 2, (j // 2) % 4, j // 8
            spot = zc[dx + dy] + yc_at[(sign * dy) % 4][dc]
            found.append({"sp": spot, "tp": xs_at[(sign * dx) % 4]})
        return found

    pairs = (
        (cia_far, cia),
        (cib_far, cib),
        (cwa_far, cwa),
        (cwb_far, cwb),
        (rga_far, rga),
        (iga_far, iga),
        (rgb_far, rgb),
        (igb_far, igb),
        (da_far, da),
        (db_far, db),
        (inc_far, inc),
        (ids_far, ids),
        (gp_far, gp),
        (pg_far, pg),
        (gia_far, gia),
        (gib_far, gib),
        (owa_far, ow.at[pl.ds(0, 256)]),
        (owb_far, ow.at[pl.ds(256, 256)]),
        (stream_far, stream),
        (gain_far, gain),
        (wg_far.at[0], wg),
        (wu_far.at[0], wu),
        (wd_far.at[0], wd),
    )
    copies = [pltpu.make_async_copy(src, dst, lsem.at[n]) for n, (src, dst) in enumerate(pairs)]
    for copy in copies:
        copy.start()
    early, middle_loads, loads = copies[:14], copies[14:16], copies[16:]

    barrier = pltpu.get_barrier_semaphore()
    for dz in range(4):
        for dy in range(4):
            for dc in range(2):
                spot = zs_at[dz] + yc_at[dy][dc]
                for dx in range(4):
                    if dz or dy or dc or dx:
                        pl.semaphore_signal(
                            barrier,
                            inc=1,
                            device_id={"sp": spot, "tp": xs_at[dx]},
                            device_id_type=MESH,
                        )

    for load in early:
        load.wait()

    for n, (a_ref, b_ref) in enumerate(((rga, rgb), (iga, igb))):
        for h in range(4):
            place = (iota((64, 256), 1) == iota((64, 256), 0) + 64 * h).astype(BF16)
            wb[n, 64 * h : 64 * h + 64, :] = dot(a_ref[h], place).astype(BF16)
        wb[2 + n] = jnp.zeros((256, 256), BF16)
        for h in range(2):
            wb[2 + n, 128 * h : 128 * h + 128, 128 * h : 128 * h + 128] = b_ref[h]

    for n in range(4):
        row = jnp.broadcast_to(inc[:, 128 * n : 128 * n + 128], (128, 128))
        incb[128 * n : 128 * n + 128, :] = row.T

    xs[0:8, :] = jnp.zeros((8, CH), F32)
    xs[8 : 8 + LEN, 0:256] = cia[...].astype(F32)
    xs[8 : 8 + LEN, 256:512] = cib[...].astype(F32)

    plus = softplus_neg(jnp.concatenate([da[...], db[...]], axis=1)) * GATE_SCALE

    def chunk(step):
        r0 = pl.multiple_of(step * 64, 64)
        jump = incb[pl.ds(r0, 64), :]
        jump = jnp.concatenate([jump, jump], axis=1)
        for side, taps in enumerate((cwa, cwb)):
            lanes = slice(256 * side, 256 * side + 256)
            window = xs[pl.ds(r0, 72), lanes]
            tap = taps[...].astype(F32)
            total = tap[0:1] * pltpu.roll(window, 3, 0)[8:]
            total = total + tap[1:2] * pltpu.roll(window, 2, 0)[8:]
            total = total + tap[2:3] * pltpu.roll(window, 1, 0)[8:]
            total = total + tap[3:4] * window[8:]
            conv = total.astype(BF16)
            rec = jax.nn.sigmoid(dot(conv, wb[2 * side]))
            admit = jax.nn.sigmoid(dot(conv, wb[2 * side + 1]))
            log = jump - rec * plus[:, lanes]
            gone = one_minus_exp(-2.0 * log)
            root = gone * lax.rsqrt(jnp.maximum(gone, 1e-37))
            h = root * admit * conv.astype(F32)
            a = jnp.exp(log)
            a3, h3 = a.reshape(8, 8, 256), h.reshape(8, 8, 256)
            at = iota((8, 8, 256), 1)
            for s in (1, 2, 4):
                ok = at >= s
                ap = jnp.where(ok, pltpu.roll(a3, s, 1), 1.0)
                hp = jnp.where(ok, pltpu.roll(h3, s, 1), 0.0)
                h3 = h3 + a3 * hp
                a3 = a3 * ap
            a8[pl.ds(r0, 64), lanes] = a3.reshape(64, 256)
            h8[pl.ds(r0, 64), lanes] = h3.reshape(64, 256)

    def later_chunks(step, carry):
        chunk(7 - step)
        return carry

    lax.fori_loop(0, 7, later_chunks, 0)

    e0r = jnp.broadcast_to(ids[0:1, :].astype(F32), (128, 128))
    e1r = jnp.broadcast_to(ids[1:2, :].astype(F32), (128, 128))
    e0, e1 = e0r.T, e1r.T
    earlier = iota((128, 128), 0) < iota((128, 128), 1)
    for n, er in enumerate((e0r, e1r)):
        hits = jnp.where(earlier & (e0 == er), 1.0, 0.0) + jnp.where(earlier & (e1 == er), 1.0, 0.0)
        rank = jnp.sum(hits, axis=0, keepdims=True).astype(jnp.int32)
        e = er[0:1].astype(jnp.int32)
        ez, ey, ec, ex = e // 32, (e // 8) % 4, (e // 4) % 2, e % 4
        dz, dy, dc, dx = (ez - z + 4) % 4, (ey - y + 4) % 4, (ec - core + 2) % 2, (ex - x + 4) % 4
        key = (((dx + dy + dz) % 4) * 32 + dy * 8 + dx * 2 + dc) * 16 + rank
        keys[n] = jnp.broadcast_to(key.astype(F32), (128, 128))
    first = gp[...] * jax.nn.sigmoid(pg[...])
    second = gp[...] * jax.nn.sigmoid(-pg[...])
    keys[2] = jnp.broadcast_to(first, (128, 128)).T
    keys[3] = jnp.broadcast_to(second, (128, 128)).T

    def pack_matrix(step, carry):
        r0 = pl.multiple_of(step * 128, 128)
        rho = (iota((128, 128), 0) + r0).astype(F32)
        k0, k1 = keys[0], keys[1]
        for q in range(4):
            hit = (rho == k0 + 4.0 * q) | (rho == k1 + 4.0 * q)
            mp[pl.ds(r0, 128), 128 * q : 128 * q + 128] = jnp.where(hit, 1.0, 0.0).astype(BF16)
        return carry

    lax.fori_loop(0, 16, pack_matrix, 0)

    pl.semaphore_wait(barrier, 127)
    nextsp = {"sp": (sp + 1) % SPN, "tp": x}
    halos = [
        pltpu.make_async_remote_copy(
            ref.at[pl.ds(LEN - 16, 16)],
            halo.at[n],
            hsem.at[n],
            hsem.at[2 + n],
            device_id=nextsp,
            device_id_type=MESH,
        )
        for n, ref in enumerate((cia, cib))
    ]
    for copy in halos:
        copy.start()

    keys[0] = keys[0].T
    keys[1] = keys[1].T

    def pick_matrix(step, carry):
        r0 = pl.multiple_of(step * 128, 128)
        c, lane = step // 4, step % 4
        rho = (iota((128, 128), 1) + r0).astype(F32)
        k0, k1, w0, w1 = keys[0], keys[1], keys[2], keys[3]
        for q in range(4):
            val = jnp.where(rho == k0 + 4.0 * q, w0, 0.0) + jnp.where(rho == k1 + 4.0 * q, w1, 0.0)
            gm[step, 128 * q : 128 * q + 128, :] = val.astype(BF16)
        return carry

    lax.fori_loop(0, 16, pick_matrix, 0)

    for load in middle_loads:
        load.wait()

    def gelus(step, carry):
        r0 = pl.multiple_of(step * 64, 64)
        gl[pl.ds(r0, 64), 0:256] = jax.nn.gelu(gia[pl.ds(r0, 64), :].astype(F32))
        gl[pl.ds(r0, 64), 256:512] = jax.nn.gelu(gib[pl.ds(r0, 64), :].astype(F32))
        return carry

    lax.fori_loop(0, 8, gelus, 0)

    for copy in halos:
        copy.wait()
    keep = jnp.where(sp > 0, 1.0, 0.0)
    xs[0:8, 0:256] = halo[0].astype(F32)[8:16] * keep
    xs[0:8, 256:512] = halo[1].astype(F32)[8:16] * keep
    chunk(0)

    def link(step, carry):
        prod, state = carry
        for n in range(8):
            r0 = pl.multiple_of(step * 64, 64) + 8 * n
            a, h = a8[pl.ds(r0, 8), :], h8[pl.ds(r0, 8), :]
            h = h + a * state
            a = a * prod
            a8[pl.ds(r0, 8), :] = a
            h8[pl.ds(r0, 8), :] = h
            prod, state = a[7:8], h[7:8]
        return prod, state

    prod, state = lax.fori_loop(0, 8, link, (jnp.ones((1, CH), F32), jnp.zeros((1, CH), F32)))
    for n in range(4):
        stat[n : n + 1, :] = prod[:, 128 * n : 128 * n + 128]
        stat[4 + n : 5 + n, :] = state[:, 128 * n : 128 * n + 128]

    for k in range(1, SPN):
        pltpu.make_async_remote_copy(
            stat,
            carry_in.at[k],
            csem.at[0],
            csem.at[1],
            device_id={"sp": lax.rem(sp + k, SPN), "tp": x},
            device_id_type=MESH,
        ).start()
    told = carry_in.at[pl.ds(1, SPN - 1)]
    pltpu.make_async_copy(told, told, csem.at[1]).wait()

    enter = jnp.zeros((4, 128), F32)
    for k in range(SPN - 1, 0, -1):
        enter = jnp.where(k <= sp, carry_in[k, 0:4] * enter + carry_in[k, 4:8], enter)
    enter = jnp.concatenate([enter[n : n + 1] for n in range(4)], axis=1)

    def hiddens(step, carry):
        r0 = pl.multiple_of(step * 64, 64)
        states = h8[pl.ds(r0, 64), :] + a8[pl.ds(r0, 64), :] * enter
        hid[pl.ds(r0, 64), :] = (states * gl[pl.ds(r0, 64), :]).astype(BF16)
        return carry

    lax.fori_loop(0, 8, hiddens, 0)

    loads[0].wait()
    loads[1].wait()

    def rows_for(d):
        return hid[pl.ds(pl.multiple_of(((x + d) % 4) * 128, 128), 128), :]

    def project(d, half, extra=None):
        rows = rows_for(d)
        for n in range(2):
            at = 1024 * half + 512 * n
            part = dot(rows, ow[:, at : at + 512])
            if extra is not None:
                part = part + extra[:, 512 * n : 512 * n + 512].astype(F32)
            psend[2 * d + half - 2, :, 512 * n : 512 * n + 512] = part.astype(BF16)

    def push(d, half, dst, sem, dx):
        copy = pltpu.make_async_remote_copy(
            psend.at[2 * d + half - 2],
            dst,
            psem.at[2 * sem],
            psem.at[2 * sem + 1],
            device_id={"sp": sp, "tp": (x + dx) % 4},
            device_id_type=MESH,
        )
        copy.start()
        return copy

    project(2, 0)
    sums = [push(2, 0, rd2.at[0], 0, 1)]
    project(2, 1)
    sums.append(push(2, 1, rd2.at[1], 1, 3))
    project(1, 1)
    sums.append(push(1, 1, prec.at[1], 2, 1))
    project(3, 0)
    sums.append(push(3, 0, prec.at[2], 3, 3))
    own = rows_for(0)
    for n in range(4):
        p0[:, 512 * n : 512 * n + 512] = dot(own, ow[:, 512 * n : 512 * n + 512])
    sums[0].wait_recv()
    project(1, 0, rd2.at[0])
    sums.append(push(1, 0, prec.at[0], 4, 1))
    sums[1].wait_recv()
    project(3, 1, rd2.at[1])
    sums.append(push(3, 1, prec.at[3], 5, 3))
    for copy in sums[2:]:
        copy.wait_recv()

    loads[2].wait()
    loads[3].wait()
    gains = gain[...].astype(F32)
    gains = jnp.concatenate([gains[n : n + 1] for n in range(16)], axis=1)

    def norms(step, carry):
        r0 = pl.multiple_of(step * 16, 16)
        rows = pl.ds(r0, 16)
        mixed = p0[rows, :]
        left = jnp.concatenate([prec[0, rows, :], prec[1, rows, :]], axis=1).astype(F32)
        right = jnp.concatenate([prec[2, rows, :], prec[3, rows, :]], axis=1).astype(F32)
        middle = (stream[rows, :].astype(F32) + (mixed + left + right)).astype(BF16).astype(F32)
        scale = lax.rsqrt(jnp.mean(middle * middle, axis=-1, keepdims=True) + EPSILON)
        normed = (middle * scale * gains).astype(BF16)
        for q in range(4):
            acc[pl.ds(128 * q + r0, 16), :] = middle[:, 512 * q : 512 * q + 512]
            nq[pl.ds(128 * q + r0, 16), :] = normed[:, 512 * q : 512 * q + 512]
        return carry

    lax.fori_loop(0, 8, norms, 0)

    def send_class(c, src, dst, sem, sign):
        for j, peer in enumerate(class_devices(c, sign)):
            tile = pl.ds(pl.multiple_of(c * 512, 512) + 16 * j, 16)
            copy = pltpu.make_async_remote_copy(
                src.at[tile],
                dst.at[tile],
                sem.at[0],
                sem.at[1 + c],
                device_id=peer,
                device_id_type=MESH,
            )
            if j == 0:
                pl.when(c > 0)(copy.start)
            else:
                copy.start()

    def dispatch(c, carry):
        for n in range(4):
            r0 = pl.multiple_of(c * 512, 512) + 128 * n
            sendb[pl.ds(r0, 128), :] = dot(mp[pl.ds(r0, 128), :], nq[...]).astype(BF16)

        send_class(c, sendb, recvb, dsem, 1)
        return carry

    lax.fori_loop(0, 4, dispatch, 0)
    recvb[0:16, :] = sendb[0:16, :]

    for load in loads[4:]:
        load.wait()

    def wait_class(buf, sem, c):
        @pl.when(c == 0)
        def _():
            part = buf.at[pl.ds(16, 496)]
            pltpu.make_async_copy(part, part, sem.at[1]).wait()

        @pl.when(c > 0)
        def _():
            part = buf.at[pl.ds(pl.multiple_of(c * 512, 512), 512)]
            pltpu.make_async_copy(part, part, sem.at[1 + c]).wait()

    def experts(c, carry):
        wait_class(recvb, dsem, c)
        ra, rb = iota((256, 256), 0), iota((256, 256), 1)
        sort = (rb == ((ra % 64) // 4) * 16 + (ra // 64) * 4 + ra % 4).astype(F32).astype(BF16)
        unsort = (ra == ((rb % 64) // 4) * 16 + (rb // 64) * 4 + rb % 4).astype(F32).astype(BF16)
        for half in range(2):
            r0 = pl.multiple_of(c * 512, 512) + 256 * half
            got = dot(sort, recvb[pl.ds(r0, 256), :]).astype(BF16)
            for q in range(4):
                xb[64 * half : 64 * half + 64, 512 * q : 512 * q + 512] = got[64 * q : 64 * q + 64]
        for n in range(4):
            cols = slice(256 * n, 256 * n + 256)
            gate = dot(xb[...], wg[:, cols])
            up = dot(xb[...], wu[:, cols])
            inner[:, cols] = (jax.nn.silu(gate) * up).astype(BF16)
        for q in range(4):
            down = dot(inner[...], wd[:, 512 * q : 512 * q + 512]).astype(BF16)
            for half in range(2):
                yb[half, 64 * q : 64 * q + 64, :] = down[64 * half : 64 * half + 64]
        for half in range(2):
            r0 = pl.multiple_of(c * 512, 512) + 256 * half
            replyb[pl.ds(r0, 256), :] = dot(unsort, yb[half]).astype(BF16)

        send_class(c, replyb, retb, rsem, -1)
        return carry

    lax.fori_loop(0, 4, experts, 0)
    retb[0:16, :] = replyb[0:16, :]

    def combine(c, carry):
        wait_class(retb, rsem, c)
        for n in range(4):
            rows = slice(128 * n, 128 * n + 128)
            part = acc[rows, :]
            for lane in range(4):
                r0 = pl.multiple_of(c * 512, 512) + 128 * lane
                part = part + dot(gm[4 * c + lane, rows, :], retb[pl.ds(r0, 128), :])
            acc[rows, :] = part
        return carry

    lax.fori_loop(0, 4, combine, 0)
    for q in range(4):
        out[:, 512 * q : 512 * q + 512] = acc[128 * q : 128 * q + 128, :].astype(BF16)

    pltpu.make_async_copy(told, told, csem.at[0]).wait()
    for copy in sums:
        copy.wait_send()
    for buf, sem in ((sendb, dsem), (replyb, rsem)):
        part = buf.at[pl.ds(16, 2032)]
        pltpu.make_async_copy(part, part, sem.at[0]).wait()


def shards(*args):
    (
        stream,
        cia,
        cib,
        gia,
        gib,
        cwa,
        cwb,
        rga,
        iga,
        rgb,
        igb,
        da,
        db,
        inc,
        owa,
        owb,
        gain,
        ids,
        gp,
        pg,
        wg,
        wu,
        wd,
    ) = args
    row = lambda a: a.reshape(1, -1)
    operands = (
        stream,
        cia,
        cib,
        gia,
        gib,
        cwa,
        cwb,
        rga,
        iga,
        rgb,
        igb,
        row(da),
        row(db),
        row(inc),
        owa,
        owb,
        gain.reshape(16, 128),
        ids.T,
        row(gp),
        row(pg),
        wg,
        wu,
        wd,
    )
    vmem = pl.BlockSpec(memory_space=pltpu.VMEM)
    far = pl.BlockSpec(memory_space=pl.ANY)
    V = pltpu.VMEM
    near = [V(a.shape, a.dtype) for n, a in enumerate(operands[:20]) if n not in (14, 15)]
    return pl.pallas_call(
        kernel,
        out_shape=pltpu.VMEM((ROWS, D), BF16),
        in_specs=[far] * len(operands),
        out_specs=vmem,
        scratch_shapes=near
        + [
            V((D, HID), BF16),
            V((D, HID), BF16),
            V((HID, D), BF16),
            V((CH, D), BF16),
            V((LEN + 8, CH), F32),
            V((4, 256, 256), BF16),
            V((LEN, 128), F32),
            V((LEN, CH), F32),
            V((LEN, CH), F32),
            V((LEN, CH), F32),
            V((LEN, CH), BF16),
            V((2, 16, 256), BF16),
            V((8, 128), F32),
            V((SPN, 8, 128), F32),
            V((6, ROWS, 1024), BF16),
            V((2, ROWS, 1024), BF16),
            V((4, ROWS, 1024), BF16),
            V((ROWS, D), F32),
            V((512, Q), BF16),
            V((2048, 512), BF16),
            V((16, 512, 128), BF16),
            V((2048, Q), BF16),
            V((2048, Q), BF16),
            V((2048, Q), BF16),
            V((2048, Q), BF16),
            V((128, D), BF16),
            V((128, HID), BF16),
            V((2, 256, Q), BF16),
            V((512, Q), F32),
            V((4, 128, 128), F32),
            pltpu.SemaphoreType.DMA((23,)),
            pltpu.SemaphoreType.DMA((4,)),
            pltpu.SemaphoreType.DMA((2,)),
            pltpu.SemaphoreType.DMA((12,)),
            pltpu.SemaphoreType.DMA((5,)),
            pltpu.SemaphoreType.DMA((5,)),
        ],
        compiler_params=pltpu.CompilerParams(
            collective_id=0, has_side_effects=True, vmem_limit_bytes=58 * 1024 * 1024
        ),
        name="layer",
    )(*operands)


def solution(mesh):
    placed = (
        P(("sp", "tp"), None),
        P("sp", "tp"),
        P("sp", "tp"),
        P("sp", "tp"),
        P("sp", "tp"),
        P(None, "tp"),
        P(None, "tp"),
        P("tp", None, None),
        P("tp", None, None),
        P("tp", None, None),
        P("tp", None, None),
        P("tp"),
        P("tp"),
        P("sp"),
        P("tp", None),
        P("tp", None),
        P(),
        P(("sp", "tp"), None),
        P(("sp", "tp")),
        P(("sp", "tp")),
        P(("sp", "tp"), None, None),
        P(("sp", "tp"), None, None),
        P(("sp", "tp"), None, None),
    )
    return jax.shard_map(
        shards, mesh=mesh, in_specs=placed, out_specs=P(("sp", "tp"), None), check_vma=False
    )
```

```python
import jax
import jax.numpy as jnp
from jax import lax
from jax.experimental import pallas as pl
from jax.experimental.pallas import tpu as pltpu
from jax.sharding import PartitionSpec as P

EPSILON = 1e-06
GATE_SCALE = 8.0
F32 = jnp.float32
BF16 = jnp.bfloat16
MESH = pl.DeviceIdType.MESH
ROWS = 128
LEN = 512
CH = 512
D = 2048
Q = 512
HID = 1024
SPN = 32


def dot(a, b):
    return jnp.dot(a, b, preferred_element_type=F32)


def iota(shape, dim):
    return lax.broadcasted_iota(jnp.int32, shape, dim)


def one_minus_square(log, a):
    u = -2.0 * log
    series = u * (1.0 - u * (0.5 - u * (1.0 / 6 - u * (1.0 / 24 - u * (1.0 / 120)))))
    return jnp.where(u < 0.05, series, 1.0 - a * a)


def softplus_neg(d):
    y = jnp.exp(-jnp.abs(d))
    w = 1.0 + y
    near = w - 1.0
    log1p = jnp.where(near == 0.0, y, jnp.log(w) * (y / jnp.where(near == 0.0, 1.0, near)))
    return jnp.maximum(-d, 0.0) + log1p


def kernel(
    stream_far,
    cia_far,
    cib_far,
    gia_far,
    gib_far,
    cwa_far,
    cwb_far,
    rga_far,
    iga_far,
    rgb_far,
    igb_far,
    da_far,
    db_far,
    inc_far,
    owa_far,
    owb_far,
    gain_far,
    ids_far,
    gp_far,
    pg_far,
    wg_far,
    wu_far,
    wd_far,
    out,
    stream,
    cia,
    cib,
    gia,
    gib,
    cwa,
    cwb,
    rga,
    iga,
    rgb,
    igb,
    da,
    db,
    inc,
    gain,
    ids,
    gp,
    pg,
    wg,
    wu,
    wd,
    ow,
    xs,
    wb,
    incb,
    a8,
    h8,
    gl,
    hid,
    halo,
    stat,
    carry_in,
    psend,
    rd2,
    prec,
    p0,
    nq,
    mp,
    gm,
    sendb,
    recvb,
    replyb,
    retb,
    xb,
    inner,
    yb,
    acc,
    keys,
    lsem,
    hsem,
    csem,
    psem,
    dsem,
    rsem,
):
    sp = lax.axis_index("sp")
    x = lax.axis_index("tp")
    z, y, core = sp // 8, (sp // 2) % 4, sp % 2

    xs_at = [lax.rem(x + n, 4) for n in range(4)]
    ys_at = [lax.rem(y + n, 4) * 2 for n in range(4)]
    zs_at = [lax.rem(z + n, 4) * 8 for n in range(4)]
    cores_at = [core, 1 - core]
    yc_at = [[ys_at[n] + cores_at[m] for m in range(2)] for n in range(4)]

    def class_devices(c, sign):
        zc = [lax.rem(z + sign * (c - n) + 16, 4) * 8 for n in range(7)]
        found = []
        for j in range(32):
            dc, dx, dy = j % 2, (j // 2) % 4, j // 8
            spot = zc[dx + dy] + yc_at[(sign * dy) % 4][dc]
            found.append({"sp": spot, "tp": xs_at[(sign * dx) % 4]})
        return found

    pairs = (
        (cia_far, cia),
        (cib_far, cib),
        (cwa_far, cwa),
        (cwb_far, cwb),
        (rga_far, rga),
        (iga_far, iga),
        (rgb_far, rgb),
        (igb_far, igb),
        (da_far, da),
        (db_far, db),
        (inc_far, inc),
        (ids_far, ids),
        (gp_far, gp),
        (pg_far, pg),
        (gia_far, gia),
        (gib_far, gib),
        (owa_far, ow.at[pl.ds(0, 256)]),
        (owb_far, ow.at[pl.ds(256, 256)]),
        (stream_far, stream),
        (gain_far, gain),
        (wg_far.at[0], wg),
        (wu_far.at[0], wu),
        (wd_far.at[0], wd),
    )
    copies = [pltpu.make_async_copy(src, dst, lsem.at[n]) for n, (src, dst) in enumerate(pairs)]
    for copy in copies:
        copy.start()
    early, middle_loads, loads = copies[:14], copies[14:16], copies[16:]

    barrier = pltpu.get_barrier_semaphore()
    for dz in range(4):
        for dy in range(4):
            for dc in range(2):
                spot = zs_at[dz] + yc_at[dy][dc]
                for dx in range(4):
                    if dz or dy or dc or dx:
                        pl.semaphore_signal(
                            barrier,
                            inc=1,
                            device_id={"sp": spot, "tp": xs_at[dx]},
                            device_id_type=MESH,
                        )

    for load in early:
        load.wait()

    for n, (a_ref, b_ref) in enumerate(((rga, rgb), (iga, igb))):
        for h in range(4):
            place = (iota((64, 256), 1) == iota((64, 256), 0) + 64 * h).astype(BF16)
            wb[n, 64 * h : 64 * h + 64, :] = dot(a_ref[h], place).astype(BF16)
        wb[2 + n] = jnp.zeros((256, 256), BF16)
        for h in range(2):
            wb[2 + n, 128 * h : 128 * h + 128, 128 * h : 128 * h + 128] = b_ref[h]

    for n in range(4):
        row = jnp.broadcast_to(inc[:, 128 * n : 128 * n + 128], (128, 128))
        incb[128 * n : 128 * n + 128, :] = row.T

    xs[0:8, :] = jnp.zeros((8, CH), F32)
    xs[8 : 8 + LEN, 0:256] = cia[...].astype(F32)
    xs[8 : 8 + LEN, 256:512] = cib[...].astype(F32)

    plus = softplus_neg(jnp.concatenate([da[...], db[...]], axis=1)) * GATE_SCALE

    def chunk(step):
        r0 = pl.multiple_of(step * 64, 64)
        jump = incb[pl.ds(r0, 64), :]
        jump = jnp.concatenate([jump, jump], axis=1)
        for side, taps in enumerate((cwa, cwb)):
            lanes = slice(256 * side, 256 * side + 256)
            window = xs[pl.ds(r0, 72), lanes]
            tap = taps[...].astype(F32)
            total = tap[0:1] * pltpu.roll(window, 3, 0)[8:]
            total = total + tap[1:2] * pltpu.roll(window, 2, 0)[8:]
            total = total + tap[2:3] * pltpu.roll(window, 1, 0)[8:]
            total = total + tap[3:4] * window[8:]
            conv = total.astype(BF16)
            rec = jax.nn.sigmoid(dot(conv, wb[2 * side]))
            admit = 0.5 * jnp.tanh(0.5 * dot(conv, wb[2 * side + 1])) + 0.5
            log = jump - rec * plus[:, lanes]
            a = jnp.exp(log)
            gone = one_minus_square(log, a)
            root = gone * lax.rsqrt(jnp.maximum(gone, 1e-37))
            h = root * admit * conv.astype(F32)
            a3, h3 = a.reshape(8, 8, 256), h.reshape(8, 8, 256)
            at = iota((8, 8, 256), 1)
            for s in (1, 2, 4):
                ok = at >= s
                ap = jnp.where(ok, pltpu.roll(a3, s, 1), 1.0)
                hp = jnp.where(ok, pltpu.roll(h3, s, 1), 0.0)
                h3 = h3 + a3 * hp
                a3 = a3 * ap
            a8[pl.ds(r0, 64), lanes] = a3.reshape(64, 256)
            h8[pl.ds(r0, 64), lanes] = h3.reshape(64, 256)

    def later_chunks(step, carry):
        chunk(7 - step)
        return carry

    lax.fori_loop(0, 4, later_chunks, 0)
    pl.semaphore_wait(barrier, 127)
    nextsp = {"sp": (sp + 1) % SPN, "tp": x}
    halos = [
        pltpu.make_async_remote_copy(
            ref.at[pl.ds(LEN - 16, 16)],
            halo.at[n],
            hsem.at[n],
            hsem.at[2 + n],
            device_id=nextsp,
            device_id_type=MESH,
        )
        for n, ref in enumerate((cia, cib))
    ]
    for copy in halos:
        copy.start()

    lax.fori_loop(4, 7, later_chunks, 0)

    for copy in halos:
        copy.wait()
    keep = jnp.where(sp > 0, 1.0, 0.0)
    xs[0:8, 0:256] = halo[0].astype(F32)[8:16] * keep
    xs[0:8, 256:512] = halo[1].astype(F32)[8:16] * keep
    chunk(0)

    def link(step, carry):
        prod, state = carry
        for n in range(8):
            r0 = pl.multiple_of(step * 64, 64) + 8 * n
            a, h = a8[pl.ds(r0, 8), :], h8[pl.ds(r0, 8), :]
            h = h + a * state
            a = a * prod
            a8[pl.ds(r0, 8), :] = a
            h8[pl.ds(r0, 8), :] = h
            prod, state = a[7:8], h[7:8]
        return prod, state

    prod, state = lax.fori_loop(0, 8, link, (jnp.ones((1, CH), F32), jnp.zeros((1, CH), F32)))
    for n in range(4):
        stat[n : n + 1, :] = prod[:, 128 * n : 128 * n + 128]
        stat[4 + n : 5 + n, :] = state[:, 128 * n : 128 * n + 128]

    for k in range(1, SPN):
        pltpu.make_async_remote_copy(
            stat,
            carry_in.at[k],
            csem.at[0],
            csem.at[1],
            device_id={"sp": lax.rem(sp + k, SPN), "tp": x},
            device_id_type=MESH,
        ).start()
    told = carry_in.at[pl.ds(1, SPN - 1)]

    e0r = jnp.broadcast_to(ids[0:1, :].astype(F32), (128, 128))
    e1r = jnp.broadcast_to(ids[1:2, :].astype(F32), (128, 128))
    e0, e1 = e0r.T, e1r.T
    earlier = iota((128, 128), 0) < iota((128, 128), 1)
    for n, er in enumerate((e0r, e1r)):
        hits = jnp.where(earlier & (e0 == er), 1.0, 0.0) + jnp.where(earlier & (e1 == er), 1.0, 0.0)
        rank = jnp.sum(hits, axis=0, keepdims=True).astype(jnp.int32)
        e = er[0:1].astype(jnp.int32)
        ez, ey, ec, ex = e // 32, (e // 8) % 4, (e // 4) % 2, e % 4
        dz, dy, dc, dx = (ez - z + 4) % 4, (ey - y + 4) % 4, (ec - core + 2) % 2, (ex - x + 4) % 4
        key = (((dx + dy + dz) % 4) * 32 + dy * 8 + dx * 2 + dc) * 16 + rank
        keys[n] = jnp.broadcast_to(key.astype(F32), (128, 128))
    first = gp[...] * jax.nn.sigmoid(pg[...])
    second = gp[...] * jax.nn.sigmoid(-pg[...])
    keys[2] = jnp.broadcast_to(first, (128, 128)).T
    keys[3] = jnp.broadcast_to(second, (128, 128)).T

    def pack_matrix(step, carry):
        r0 = pl.multiple_of(step * 128, 128)
        rho = (iota((128, 128), 0) + r0).astype(F32)
        k0, k1 = keys[0], keys[1]
        for q in range(4):
            hit = (rho == k0 + 4.0 * q) | (rho == k1 + 4.0 * q)
            mp[pl.ds(r0, 128), 128 * q : 128 * q + 128] = jnp.where(hit, 1.0, 0.0).astype(BF16)
        return carry

    lax.fori_loop(0, 16, pack_matrix, 0)

    keys[0] = keys[0].T
    keys[1] = keys[1].T

    def pick_matrix(step, carry):
        r0 = pl.multiple_of(step * 128, 128)
        c, lane = step // 4, step % 4
        rho = (iota((128, 128), 1) + r0).astype(F32)
        k0, k1, w0, w1 = keys[0], keys[1], keys[2], keys[3]
        for q in range(4):
            val = jnp.where(rho == k0 + 4.0 * q, w0, 0.0) + jnp.where(rho == k1 + 4.0 * q, w1, 0.0)
            gm[step, 128 * q : 128 * q + 128, :] = val.astype(BF16)
        return carry

    lax.fori_loop(0, 16, pick_matrix, 0)

    for load in middle_loads:
        load.wait()

    def gelus(step, carry):
        r0 = pl.multiple_of(step * 64, 64)
        gl[pl.ds(r0, 64), 0:256] = jax.nn.gelu(gia[pl.ds(r0, 64), :].astype(F32))
        gl[pl.ds(r0, 64), 256:512] = jax.nn.gelu(gib[pl.ds(r0, 64), :].astype(F32))
        return carry

    lax.fori_loop(0, 8, gelus, 0)

    pltpu.make_async_copy(told, told, csem.at[1]).wait()

    enter = jnp.zeros((4, 128), F32)
    for k in range(SPN - 1, 0, -1):
        enter = jnp.where(k <= sp, carry_in[k, 0:4] * enter + carry_in[k, 4:8], enter)
    enter = jnp.concatenate([enter[n : n + 1] for n in range(4)], axis=1)

    def hiddens(step, carry):
        r0 = pl.multiple_of(lax.rem(step + 2 * x + 4, 8) * 64, 64)
        states = h8[pl.ds(r0, 64), :] + a8[pl.ds(r0, 64), :] * enter
        hid[pl.ds(r0, 64), :] = (states * gl[pl.ds(r0, 64), :]).astype(BF16)
        return carry

    loads[0].wait()
    loads[1].wait()
    lax.fori_loop(0, 2, hiddens, 0)

    def rows_for(d):
        return hid[pl.ds(pl.multiple_of(((x + d) % 4) * 128, 128), 128), :]

    def project(d, half, extra=None):
        rows = rows_for(d)
        for n in range(2):
            at = 1024 * half + 512 * n
            part = dot(rows, ow[:, at : at + 512])
            if extra is not None:
                part = part + extra[:, 512 * n : 512 * n + 512].astype(F32)
            psend[2 * d + half - 2, :, 512 * n : 512 * n + 512] = part.astype(BF16)

    def push(d, half, dst, sem, dx):
        copy = pltpu.make_async_remote_copy(
            psend.at[2 * d + half - 2],
            dst,
            psem.at[2 * sem],
            psem.at[2 * sem + 1],
            device_id={"sp": sp, "tp": (x + dx) % 4},
            device_id_type=MESH,
        )
        copy.start()
        return copy

    project(2, 0)
    sums = [push(2, 0, rd2.at[0], 0, 1)]
    project(2, 1)
    sums.append(push(2, 1, rd2.at[1], 1, 3))
    lax.fori_loop(2, 8, hiddens, 0)
    project(1, 1)
    sums.append(push(1, 1, prec.at[1], 2, 1))
    project(3, 0)
    sums.append(push(3, 0, prec.at[2], 3, 3))
    own = rows_for(0)
    for n in range(4):
        p0[:, 512 * n : 512 * n + 512] = dot(own, ow[:, 512 * n : 512 * n + 512])
    sums[0].wait_recv()
    project(1, 0, rd2.at[0])
    sums.append(push(1, 0, prec.at[0], 4, 1))
    sums[1].wait_recv()
    project(3, 1, rd2.at[1])
    sums.append(push(3, 1, prec.at[3], 5, 3))
    loads[2].wait()
    loads[3].wait()
    for copy in sums[2:4]:
        copy.wait_recv()

    def gather(step, carry):
        rows = pl.ds(pl.multiple_of(step * 16, 16), 16)
        part = jnp.concatenate([prec[2, rows, :], prec[1, rows, :]], axis=1).astype(F32)
        p0[rows, :] = p0[rows, :] + part + stream[rows, :].astype(F32)
        return carry

    lax.fori_loop(0, 8, gather, 0)
    for copy in sums[4:]:
        copy.wait_recv()
    gains = gain[...].astype(F32)
    gains = jnp.concatenate([gains[n : n + 1] for n in range(16)], axis=1)

    def norms(step, carry):
        r0 = pl.multiple_of(step * 16, 16)
        rows = pl.ds(r0, 16)
        part = jnp.concatenate([prec[0, rows, :], prec[3, rows, :]], axis=1).astype(F32)
        middle = (p0[rows, :] + part).astype(BF16).astype(F32)
        scale = lax.rsqrt(jnp.mean(middle * middle, axis=-1, keepdims=True) + EPSILON)
        normed = (middle * scale * gains).astype(BF16)
        for q in range(4):
            acc[pl.ds(128 * q + r0, 16), :] = middle[:, 512 * q : 512 * q + 512]
            nq[pl.ds(128 * q + r0, 16), :] = normed[:, 512 * q : 512 * q + 512]
        return carry

    lax.fori_loop(0, 8, norms, 0)

    def send_class(c, src, dst, sem, sign):
        for j, peer in enumerate(class_devices(c, sign)):
            tile = pl.ds(pl.multiple_of(c * 512, 512) + 16 * j, 16)
            copy = pltpu.make_async_remote_copy(
                src.at[tile],
                dst.at[tile],
                sem.at[0],
                sem.at[1 + c],
                device_id=peer,
                device_id_type=MESH,
            )
            if j == 0:
                pl.when(c > 0)(copy.start)
            else:
                copy.start()

    def dispatch(c, carry):
        for n in range(4):
            r0 = pl.multiple_of(c * 512, 512) + 128 * n
            sendb[pl.ds(r0, 128), :] = dot(mp[pl.ds(r0, 128), :], nq[...]).astype(BF16)

        send_class(c, sendb, recvb, dsem, 1)
        return carry

    lax.fori_loop(0, 4, dispatch, 0)
    recvb[0:16, :] = sendb[0:16, :]

    for load in loads[4:]:
        load.wait()

    def wait_class(buf, sem, c):
        @pl.when(c == 0)
        def _():
            part = buf.at[pl.ds(16, 496)]
            pltpu.make_async_copy(part, part, sem.at[1]).wait()

        @pl.when(c > 0)
        def _():
            part = buf.at[pl.ds(pl.multiple_of(c * 512, 512), 512)]
            pltpu.make_async_copy(part, part, sem.at[1 + c]).wait()

    def experts(c, carry):
        wait_class(recvb, dsem, c)
        ra, rb = iota((256, 256), 0), iota((256, 256), 1)
        sort = (rb == ((ra % 64) // 4) * 16 + (ra // 64) * 4 + ra % 4).astype(F32).astype(BF16)
        unsort = (ra == ((rb % 64) // 4) * 16 + (rb // 64) * 4 + rb % 4).astype(F32).astype(BF16)
        for half in range(2):
            r0 = pl.multiple_of(c * 512, 512) + 256 * half
            got = dot(sort, recvb[pl.ds(r0, 256), :]).astype(BF16)
            for q in range(4):
                xb[64 * half : 64 * half + 64, 512 * q : 512 * q + 512] = got[64 * q : 64 * q + 64]
        for n in range(4):
            cols = slice(256 * n, 256 * n + 256)
            gate = dot(xb[...], wg[:, cols])
            up = dot(xb[...], wu[:, cols])
            inner[:, cols] = (jax.nn.silu(gate) * up).astype(BF16)
        for q in range(4):
            down = dot(inner[...], wd[:, 512 * q : 512 * q + 512]).astype(BF16)
            for half in range(2):
                yb[half, 64 * q : 64 * q + 64, :] = down[64 * half : 64 * half + 64]
        for half in range(2):
            r0 = pl.multiple_of(c * 512, 512) + 256 * half
            replyb[pl.ds(r0, 256), :] = dot(unsort, yb[half]).astype(BF16)

        send_class(c, replyb, retb, rsem, -1)
        return carry

    lax.fori_loop(0, 4, experts, 0)
    retb[0:16, :] = replyb[0:16, :]

    def combine(c, carry):
        wait_class(retb, rsem, c)
        for n in range(4):
            rows = slice(128 * n, 128 * n + 128)
            part = acc[rows, :]
            for lane in range(4):
                r0 = pl.multiple_of(c * 512, 512) + 128 * lane
                part = part + dot(gm[4 * c + lane, rows, :], retb[pl.ds(r0, 128), :])
            acc[rows, :] = part
        return carry

    lax.fori_loop(0, 4, combine, 0)
    for q in range(4):
        out[:, 512 * q : 512 * q + 512] = acc[128 * q : 128 * q + 128, :].astype(BF16)

    pltpu.make_async_copy(told, told, csem.at[0]).wait()
    for copy in sums:
        copy.wait_send()
    for buf, sem in ((sendb, dsem), (replyb, rsem)):
        part = buf.at[pl.ds(16, 2032)]
        pltpu.make_async_copy(part, part, sem.at[0]).wait()


def shards(*args):
    (
        stream,
        cia,
        cib,
        gia,
        gib,
        cwa,
        cwb,
        rga,
        iga,
        rgb,
        igb,
        da,
        db,
        inc,
        owa,
        owb,
        gain,
        ids,
        gp,
        pg,
        wg,
        wu,
        wd,
    ) = args
    row = lambda a: a.reshape(1, -1)
    operands = (
        stream,
        cia,
        cib,
        gia,
        gib,
        cwa,
        cwb,
        rga,
        iga,
        rgb,
        igb,
        row(da),
        row(db),
        row(inc),
        owa,
        owb,
        gain.reshape(16, 128),
        ids.T,
        row(gp),
        row(pg),
        wg,
        wu,
        wd,
    )
    vmem = pl.BlockSpec(memory_space=pltpu.VMEM)
    far = pl.BlockSpec(memory_space=pl.ANY)
    V = pltpu.VMEM
    near = [V(a.shape, a.dtype) for n, a in enumerate(operands[:20]) if n not in (14, 15)]
    return pl.pallas_call(
        kernel,
        out_shape=pltpu.VMEM((ROWS, D), BF16),
        in_specs=[far] * len(operands),
        out_specs=vmem,
        scratch_shapes=near
        + [
            V((D, HID), BF16),
            V((D, HID), BF16),
            V((HID, D), BF16),
            V((CH, D), BF16),
            V((LEN + 8, CH), F32),
            V((4, 256, 256), BF16),
            V((LEN, 128), F32),
            V((LEN, CH), F32),
            V((LEN, CH), F32),
            V((LEN, CH), F32),
            V((LEN, CH), BF16),
            V((2, 16, 256), BF16),
            V((8, 128), F32),
            V((SPN, 8, 128), F32),
            V((6, ROWS, 1024), BF16),
            V((2, ROWS, 1024), BF16),
            V((4, ROWS, 1024), BF16),
            V((ROWS, D), F32),
            V((512, Q), BF16),
            V((2048, 512), BF16),
            V((16, 512, 128), BF16),
            V((2048, Q), BF16),
            V((2048, Q), BF16),
            V((2048, Q), BF16),
            V((2048, Q), BF16),
            V((128, D), BF16),
            V((128, HID), BF16),
            V((2, 256, Q), BF16),
            V((512, Q), F32),
            V((4, 128, 128), F32),
            pltpu.SemaphoreType.DMA((23,)),
            pltpu.SemaphoreType.DMA((4,)),
            pltpu.SemaphoreType.DMA((2,)),
            pltpu.SemaphoreType.DMA((12,)),
            pltpu.SemaphoreType.DMA((5,)),
            pltpu.SemaphoreType.DMA((5,)),
        ],
        compiler_params=pltpu.CompilerParams(
            collective_id=0, has_side_effects=True, vmem_limit_bytes=58 * 1024 * 1024
        ),
        name="layer",
    )(*operands)


def solution(mesh):
    placed = (
        P(("sp", "tp"), None),
        P("sp", "tp"),
        P("sp", "tp"),
        P("sp", "tp"),
        P("sp", "tp"),
        P(None, "tp"),
        P(None, "tp"),
        P("tp", None, None),
        P("tp", None, None),
        P("tp", None, None),
        P("tp", None, None),
        P("tp"),
        P("tp"),
        P("sp"),
        P("tp", None),
        P("tp", None),
        P(),
        P(("sp", "tp"), None),
        P(("sp", "tp")),
        P(("sp", "tp")),
        P(("sp", "tp"), None, None),
        P(("sp", "tp"), None, None),
        P(("sp", "tp"), None, None),
    )
    return jax.shard_map(
        shards, mesh=mesh, in_specs=placed, out_specs=P(("sp", "tp"), None), check_vma=False
    )
```

```python
import random

import jax
import jax.numpy as jnp
from jax import lax
from jax.experimental import pallas as pl
from jax.experimental.pallas import tpu as pltpu
from jax.sharding import PartitionSpec as P

EPSILON = 1e-06
GATE_SCALE = 8.0
F32 = jnp.float32
BF16 = jnp.bfloat16
MESH = pl.DeviceIdType.MESH
ROWS = 128
LEN = 512
CH = 512
D = 2048
Q = 512
HID = 1024
SPN = 32


def dot(a, b):
    return jnp.dot(a, b, preferred_element_type=F32)


def iota(shape, dim):
    return lax.broadcasted_iota(jnp.int32, shape, dim)


def one_minus_square(log, a):
    u = -2.0 * log
    series = u * (1.0 - u * (0.5 - u * (1.0 / 6 - u * (1.0 / 24 - u * (1.0 / 120)))))
    return jnp.where(u < 0.05, series, 1.0 - a * a)


def softplus_neg(d):
    y = jnp.exp(-jnp.abs(d))
    w = 1.0 + y
    near = w - 1.0
    log1p = jnp.where(near == 0.0, y, jnp.log(w) * (y / jnp.where(near == 0.0, 1.0, near)))
    return jnp.maximum(-d, 0.0) + log1p


def hops(step):
    return -sum(min(n, 4 - n) for n in (step[0], step[1], step[3]))


def class_steps(c, seed):
    steps = []
    for j in range(32):
        dc, dx, dy = j % 2, (j // 2) % 4, j // 8
        steps.append((j, ((c - dx - dy) % 4, dy, dc, dx)))
    steps = [s for s in steps if any(s[1])]
    random.Random(seed).shuffle(steps)
    return steps


SENDS = [class_steps(c, c + 1) for c in range(4)]
REPLIES = [class_steps(c, c + 77) for c in range(4)]


def kernel(
    stream_far,
    cia_far,
    cib_far,
    gia_far,
    gib_far,
    cwa_far,
    cwb_far,
    rga_far,
    iga_far,
    rgb_far,
    igb_far,
    da_far,
    db_far,
    inc_far,
    owa_far,
    owb_far,
    gain_far,
    ids_far,
    gp_far,
    pg_far,
    wg_far,
    wu_far,
    wd_far,
    out,
    stream,
    cia,
    cib,
    gia,
    gib,
    cwa,
    cwb,
    rga,
    iga,
    rgb,
    igb,
    da,
    db,
    inc,
    gain,
    ids,
    gp,
    pg,
    wg,
    wu,
    wd,
    ow,
    xs,
    wb,
    incb,
    a8,
    h8,
    gl,
    hid,
    halo,
    stat,
    carry_in,
    psend,
    rd2,
    prec,
    p0,
    nq,
    mp,
    gm,
    sendb,
    recvb,
    replyb,
    retb,
    xb,
    inner,
    yb,
    acc,
    keys,
    lsem,
    hsem,
    csem,
    psem,
    dsem,
    rsem,
):
    sp = lax.axis_index("sp")
    x = lax.axis_index("tp")
    z, y, core = sp // 8, (sp // 2) % 4, sp % 2

    xs_at = [lax.rem(x + n, 4) for n in range(4)]
    ys_at = [lax.rem(y + n, 4) * 2 for n in range(4)]
    zs_at = [lax.rem(z + n, 4) * 8 for n in range(4)]
    cores_at = [core, 1 - core]
    yc_at = [[ys_at[n] + cores_at[m] for m in range(2)] for n in range(4)]

    def peer(step, sign=1):
        dz, dy, dc, dx = (sign * n for n in step)
        return {"sp": zs_at[dz % 4] + yc_at[dy % 4][dc % 2], "tp": xs_at[dx % 4]}

    barrier = pltpu.get_barrier_semaphore()
    for step in sorted((step for steps in SENDS for _, step in steps), key=hops):
        pl.semaphore_signal(barrier, inc=1, device_id=peer(step), device_id_type=MESH)
    pairs = (
        (cia_far, cia),
        (cib_far, cib),
        (cwa_far, cwa),
        (cwb_far, cwb),
        (rga_far, rga),
        (iga_far, iga),
        (rgb_far, rgb),
        (igb_far, igb),
        (da_far, da),
        (db_far, db),
        (inc_far, inc),
        (ids_far, ids),
        (gp_far, gp),
        (pg_far, pg),
        (gia_far, gia),
        (gib_far, gib),
        (owa_far, ow.at[pl.ds(0, 256)]),
        (owb_far, ow.at[pl.ds(256, 256)]),
        (stream_far, stream),
        (gain_far, gain),
        (wg_far.at[0], wg),
        (wu_far.at[0], wu),
        (wd_far.at[0], wd),
    )
    copies = [pltpu.make_async_copy(src, dst, lsem.at[n]) for n, (src, dst) in enumerate(pairs)]
    for copy in copies:
        copy.start()
    early, middle_loads, loads = copies[:14], copies[14:16], copies[16:]

    for load in early:
        load.wait()

    for n, (a_ref, b_ref) in enumerate(((rga, rgb), (iga, igb))):
        for h in range(4):
            place = (iota((64, 256), 1) == iota((64, 256), 0) + 64 * h).astype(BF16)
            wb[n, 64 * h : 64 * h + 64, :] = dot(a_ref[h], place).astype(BF16)
        wb[2 + n] = jnp.zeros((256, 256), BF16)
        for h in range(2):
            wb[2 + n, 128 * h : 128 * h + 128, 128 * h : 128 * h + 128] = b_ref[h]

    for n in range(4):
        row = jnp.broadcast_to(inc[:, 128 * n : 128 * n + 128], (128, 128))
        incb[128 * n : 128 * n + 128, :] = row.T

    xs[0:8, :] = jnp.zeros((8, CH), F32)
    xs[8 : 8 + LEN, 0:256] = cia[...].astype(F32)
    xs[8 : 8 + LEN, 256:512] = cib[...].astype(F32)

    plus = softplus_neg(jnp.concatenate([da[...], db[...]], axis=1)) * GATE_SCALE

    def chunk(step):
        r0 = pl.multiple_of(step * 64, 64)
        jump = incb[pl.ds(r0, 64), :]
        jump = jnp.concatenate([jump, jump], axis=1)
        for side, taps in enumerate((cwa, cwb)):
            lanes = slice(256 * side, 256 * side + 256)
            window = xs[pl.ds(r0, 72), lanes]
            tap = taps[...].astype(F32)
            total = tap[0:1] * pltpu.roll(window, 3, 0)[8:]
            total = total + tap[1:2] * pltpu.roll(window, 2, 0)[8:]
            total = total + tap[2:3] * pltpu.roll(window, 1, 0)[8:]
            total = total + tap[3:4] * window[8:]
            conv = total.astype(BF16)
            rec = jax.nn.sigmoid(dot(conv, wb[2 * side]))
            admit = 0.5 * jnp.tanh(0.5 * dot(conv, wb[2 * side + 1])) + 0.5
            log = jump - rec * plus[:, lanes]
            a = jnp.exp(log)
            gone = one_minus_square(log, a)
            root = gone * lax.rsqrt(jnp.maximum(gone, 1e-37))
            h = root * admit * conv.astype(F32)
            a3, h3 = a.reshape(8, 8, 256), h.reshape(8, 8, 256)
            at = iota((8, 8, 256), 1)
            for s in (1, 2, 4):
                ok = at >= s
                ap = jnp.where(ok, pltpu.roll(a3, s, 1), 1.0)
                hp = jnp.where(ok, pltpu.roll(h3, s, 1), 0.0)
                h3 = h3 + a3 * hp
                a3 = a3 * ap
            a8[pl.ds(r0, 64), lanes] = a3.reshape(64, 256)
            h8[pl.ds(r0, 64), lanes] = h3.reshape(64, 256)

    def later_chunks(step, carry):
        chunk(7 - step)
        return carry

    lax.fori_loop(0, 4, later_chunks, 0)
    pl.semaphore_wait(barrier, 127)
    nextsp = {"sp": (sp + 1) % SPN, "tp": x}
    halos = [
        pltpu.make_async_remote_copy(
            ref.at[pl.ds(LEN - 16, 16)],
            halo.at[n],
            hsem.at[n],
            hsem.at[2 + n],
            device_id=nextsp,
            device_id_type=MESH,
        )
        for n, ref in enumerate((cia, cib))
    ]
    for copy in halos:
        copy.start()

    lax.fori_loop(4, 7, later_chunks, 0)

    for copy in halos:
        copy.wait()
    keep = jnp.where(sp > 0, 1.0, 0.0)
    xs[0:8, 0:256] = halo[0].astype(F32)[8:16] * keep
    xs[0:8, 256:512] = halo[1].astype(F32)[8:16] * keep
    chunk(0)

    def link(step, carry):
        prod, state = carry
        for n in range(8):
            r0 = pl.multiple_of(step * 64, 64) + 8 * n
            a, h = a8[pl.ds(r0, 8), :], h8[pl.ds(r0, 8), :]
            h = h + a * state
            a = a * prod
            a8[pl.ds(r0, 8), :] = a
            h8[pl.ds(r0, 8), :] = h
            prod, state = a[7:8], h[7:8]
        return prod, state

    prod, state = lax.fori_loop(0, 8, link, (jnp.ones((1, CH), F32), jnp.zeros((1, CH), F32)))
    for n in range(4):
        stat[n : n + 1, :] = prod[:, 128 * n : 128 * n + 128]
        stat[4 + n : 5 + n, :] = state[:, 128 * n : 128 * n + 128]

    for k in range(1, SPN):
        pltpu.make_async_remote_copy(
            stat,
            carry_in.at[k],
            csem.at[0],
            csem.at[1],
            device_id={"sp": lax.rem(sp + k, SPN), "tp": x},
            device_id_type=MESH,
        ).start()
    told = carry_in.at[pl.ds(1, SPN - 1)]

    e0r = jnp.broadcast_to(ids[0:1, :].astype(F32), (128, 128))
    e1r = jnp.broadcast_to(ids[1:2, :].astype(F32), (128, 128))
    e0, e1 = e0r.T, e1r.T
    earlier = iota((128, 128), 0) < iota((128, 128), 1)
    for n, er in enumerate((e0r, e1r)):
        hits = jnp.where(earlier & (e0 == er), 1.0, 0.0) + jnp.where(earlier & (e1 == er), 1.0, 0.0)
        rank = jnp.sum(hits, axis=0, keepdims=True).astype(jnp.int32)
        e = er[0:1].astype(jnp.int32)
        ez, ey, ec, ex = e // 32, (e // 8) % 4, (e // 4) % 2, e % 4
        dz, dy, dc, dx = (ez - z + 4) % 4, (ey - y + 4) % 4, (ec - core + 2) % 2, (ex - x + 4) % 4
        key = (((dx + dy + dz) % 4) * 32 + dy * 8 + dx * 2 + dc) * 16 + rank
        keys[n] = jnp.broadcast_to(key.astype(F32), (128, 128))
    first = gp[...] * jax.nn.sigmoid(pg[...])
    second = gp[...] * jax.nn.sigmoid(-pg[...])
    keys[2] = jnp.broadcast_to(first, (128, 128)).T
    keys[3] = jnp.broadcast_to(second, (128, 128)).T

    def pack_matrix(step, carry):
        r0 = pl.multiple_of(step * 128, 128)
        rho = (iota((128, 128), 0) + r0).astype(F32)
        k0, k1 = keys[0], keys[1]
        for q in range(4):
            hit = (rho == k0 + 4.0 * q) | (rho == k1 + 4.0 * q)
            mp[pl.ds(r0, 128), 128 * q : 128 * q + 128] = jnp.where(hit, 1.0, 0.0).astype(BF16)
        return carry

    lax.fori_loop(0, 16, pack_matrix, 0)

    keys[0] = keys[0].T
    keys[1] = keys[1].T

    def pick_matrix(c, carry):
        k0, k1, w0, w1 = keys[0], keys[1], keys[2], keys[3]
        for lane in range(4):
            rho = (iota((128, 128), 1) + (c * 512 + 128 * lane)).astype(F32)
            cols = slice(128 * lane, 128 * lane + 128)
            for q in range(4):
                val = jnp.where(rho == k0 + 4.0 * q, w0, 0.0)
                val = val + jnp.where(rho == k1 + 4.0 * q, w1, 0.0)
                gm[c, 128 * q : 128 * q + 128, cols] = val.astype(BF16)
        return carry

    lax.fori_loop(0, 4, pick_matrix, 0)

    for load in middle_loads:
        load.wait()

    def gelus(step, carry):
        r0 = pl.multiple_of(step * 64, 64)
        gl[pl.ds(r0, 64), 0:256] = jax.nn.gelu(gia[pl.ds(r0, 64), :].astype(F32))
        gl[pl.ds(r0, 64), 256:512] = jax.nn.gelu(gib[pl.ds(r0, 64), :].astype(F32))
        return carry

    lax.fori_loop(0, 8, gelus, 0)

    pltpu.make_async_copy(told, told, csem.at[1]).wait()

    enter = jnp.zeros((4, 128), F32)
    for k in range(SPN - 1, 0, -1):
        enter = jnp.where(k <= sp, carry_in[k, 0:4] * enter + carry_in[k, 4:8], enter)
    enter = jnp.concatenate([enter[n : n + 1] for n in range(4)], axis=1)

    def hiddens(step, carry):
        r0 = pl.multiple_of(lax.rem(step + 2 * x + 4, 8) * 64, 64)
        states = h8[pl.ds(r0, 64), :] + a8[pl.ds(r0, 64), :] * enter
        hid[pl.ds(r0, 64), :] = (states * gl[pl.ds(r0, 64), :]).astype(BF16)
        return carry

    loads[0].wait()
    loads[1].wait()
    lax.fori_loop(0, 2, hiddens, 0)

    def rows_for(d):
        return hid[pl.ds(pl.multiple_of(((x + d) % 4) * 128, 128), 128), :]

    def project(d, half, extra=None):
        rows = rows_for(d)
        for n in range(2):
            at = 1024 * half + 512 * n
            part = dot(rows, ow[:, at : at + 512])
            if extra is not None:
                part = part + extra[:, 512 * n : 512 * n + 512].astype(F32)
            psend[2 * d + half - 2, :, 512 * n : 512 * n + 512] = part.astype(BF16)

    def push(d, half, dst, sem, dx):
        copy = pltpu.make_async_remote_copy(
            psend.at[2 * d + half - 2],
            dst,
            psem.at[2 * sem],
            psem.at[2 * sem + 1],
            device_id={"sp": sp, "tp": (x + dx) % 4},
            device_id_type=MESH,
        )
        copy.start()
        return copy

    project(2, 0)
    sums = [push(2, 0, rd2.at[0], 0, 1)]
    project(2, 1)
    sums.append(push(2, 1, rd2.at[1], 1, 3))
    lax.fori_loop(2, 8, hiddens, 0)
    project(1, 1)
    sums.append(push(1, 1, prec.at[1], 2, 1))
    project(3, 0)
    sums.append(push(3, 0, prec.at[2], 3, 3))
    own = rows_for(0)
    for n in range(4):
        p0[:, 512 * n : 512 * n + 512] = dot(own, ow[:, 512 * n : 512 * n + 512])
    sums[0].wait_recv()
    project(1, 0, rd2.at[0])
    sums.append(push(1, 0, prec.at[0], 4, 1))
    sums[1].wait_recv()
    project(3, 1, rd2.at[1])
    sums.append(push(3, 1, prec.at[3], 5, 3))
    loads[2].wait()
    loads[3].wait()
    for copy in sums[2:4]:
        copy.wait_recv()

    def gather(step, carry):
        rows = pl.ds(pl.multiple_of(step * 16, 16), 16)
        part = jnp.concatenate([prec[2, rows, :], prec[1, rows, :]], axis=1).astype(F32)
        p0[rows, :] = p0[rows, :] + part + stream[rows, :].astype(F32)
        return carry

    lax.fori_loop(0, 8, gather, 0)
    for copy in sums[4:]:
        copy.wait_recv()
    gains = gain[...].astype(F32)
    gains = jnp.concatenate([gains[n : n + 1] for n in range(16)], axis=1)

    def norms(step, carry):
        r0 = pl.multiple_of(step * 16, 16)
        rows = pl.ds(r0, 16)
        part = jnp.concatenate([prec[0, rows, :], prec[3, rows, :]], axis=1).astype(F32)
        middle = (p0[rows, :] + part).astype(BF16).astype(F32)
        scale = lax.rsqrt(jnp.mean(middle * middle, axis=-1, keepdims=True) + EPSILON)
        normed = (middle * scale * gains).astype(BF16)
        for q in range(4):
            acc[pl.ds(128 * q + r0, 16), :] = middle[:, 512 * q : 512 * q + 512]
            nq[pl.ds(128 * q + r0, 16), :] = normed[:, 512 * q : 512 * q + 512]
        return carry

    lax.fori_loop(0, 8, norms, 0, unroll=4)

    def send_class(c, src, dst, sem, sign):
        for n, steps in enumerate(SENDS if sign > 0 else REPLIES):

            @pl.when(c == n)
            def _(n=n, steps=steps):
                for j, step in steps:
                    tile = pl.ds(512 * n + 16 * j, 16)
                    pltpu.make_async_remote_copy(
                        src.at[tile],
                        dst.at[tile],
                        sem.at[0],
                        sem.at[1 + n],
                        device_id=peer(step, sign),
                        device_id_type=MESH,
                    ).start()

    def dispatch(c, carry):
        for n in range(4):
            r0 = pl.multiple_of(c * 512, 512) + 128 * n
            sendb[pl.ds(r0, 128), :] = dot(mp[pl.ds(r0, 128), :], nq[...]).astype(BF16)

        send_class(c, sendb, recvb, dsem, 1)
        return carry

    lax.fori_loop(0, 4, dispatch, 0)
    recvb[0:16, :] = sendb[0:16, :]

    for load in loads[4:]:
        load.wait()

    def wait_class(buf, sem, c):
        if isinstance(c, int):
            part = buf.at[pl.ds(c * 512, 512)]
            pltpu.make_async_copy(part, part, sem.at[1 + c]).wait()
            return

        @pl.when(c == 0)
        def _():
            part = buf.at[pl.ds(16, 496)]
            pltpu.make_async_copy(part, part, sem.at[1]).wait()

        @pl.when(c > 0)
        def _():
            part = buf.at[pl.ds(pl.multiple_of(c * 512, 512), 512)]
            pltpu.make_async_copy(part, part, sem.at[1 + c]).wait()

    def experts(c, carry):
        wait_class(recvb, dsem, c)
        ra, rb = iota((256, 256), 0), iota((256, 256), 1)
        sort = (rb == ((ra % 64) // 4) * 16 + (ra // 64) * 4 + ra % 4).astype(F32).astype(BF16)
        unsort = (ra == ((rb % 64) // 4) * 16 + (rb // 64) * 4 + rb % 4).astype(F32).astype(BF16)
        for half in range(2):
            r0 = pl.multiple_of(c * 512, 512) + 256 * half
            got = dot(sort, recvb[pl.ds(r0, 256), :]).astype(BF16)
            for q in range(4):
                xb[64 * half : 64 * half + 64, 512 * q : 512 * q + 512] = got[64 * q : 64 * q + 64]
        for n in range(4):
            cols = slice(256 * n, 256 * n + 256)
            gate = dot(xb[...], wg[:, cols])
            up = dot(xb[...], wu[:, cols])
            inner[:, cols] = (jax.nn.silu(gate) * up).astype(BF16)
        for q in range(4):
            down = dot(inner[...], wd[:, 512 * q : 512 * q + 512]).astype(BF16)
            for half in range(2):
                yb[half, 64 * q : 64 * q + 64, :] = down[64 * half : 64 * half + 64]
        for half in range(2):
            r0 = pl.multiple_of(c * 512, 512) + 256 * half
            replyb[pl.ds(r0, 256), :] = dot(unsort, yb[half]).astype(BF16)

        send_class(c, replyb, retb, rsem, -1)
        return carry

    lax.fori_loop(0, 4, experts, 0)
    retb[0:16, :] = replyb[0:16, :]

    def combine(c, carry):
        wait_class(retb, rsem, c)
        got = pl.ds(pl.multiple_of(c * 512, 512), 512)
        for n in range(4):
            rows = slice(128 * n, 128 * n + 128)
            acc[rows, :] = acc[rows, :] + dot(gm[c, rows, :], retb[got, :])
        return carry

    lax.fori_loop(0, 3, combine, 0)
    wait_class(retb, rsem, 3)
    for q in range(4):
        rows = slice(128 * q, 128 * q + 128)
        total = acc[rows, :] + dot(gm[3, rows, :], retb[1536:2048, :])
        out[:, 512 * q : 512 * q + 512] = total.astype(BF16)

    pltpu.make_async_copy(told, told, csem.at[0]).wait()
    for copy in sums:
        copy.wait_send()
    for buf, sem in ((sendb, dsem), (replyb, rsem)):
        part = buf.at[pl.ds(16, 2032)]
        pltpu.make_async_copy(part, part, sem.at[0]).wait()


def shards(*args):
    (
        stream,
        cia,
        cib,
        gia,
        gib,
        cwa,
        cwb,
        rga,
        iga,
        rgb,
        igb,
        da,
        db,
        inc,
        owa,
        owb,
        gain,
        ids,
        gp,
        pg,
        wg,
        wu,
        wd,
    ) = args
    row = lambda a: a.reshape(1, -1)
    operands = (
        stream,
        cia,
        cib,
        gia,
        gib,
        cwa,
        cwb,
        rga,
        iga,
        rgb,
        igb,
        row(da),
        row(db),
        row(inc),
        owa,
        owb,
        gain.reshape(16, 128),
        ids.T,
        row(gp),
        row(pg),
        wg,
        wu,
        wd,
    )
    vmem = pl.BlockSpec(memory_space=pltpu.VMEM)
    far = pl.BlockSpec(memory_space=pl.ANY)
    V = pltpu.VMEM
    near = [V(a.shape, a.dtype) for n, a in enumerate(operands[:20]) if n not in (14, 15)]
    return pl.pallas_call(
        kernel,
        out_shape=pltpu.VMEM((ROWS, D), BF16),
        in_specs=[far] * len(operands),
        out_specs=vmem,
        scratch_shapes=near
        + [
            V((D, HID), BF16),
            V((D, HID), BF16),
            V((HID, D), BF16),
            V((CH, D), BF16),
            V((LEN + 8, CH), F32),
            V((4, 256, 256), BF16),
            V((LEN, 128), F32),
            V((LEN, CH), F32),
            V((LEN, CH), F32),
            V((LEN, CH), F32),
            V((LEN, CH), BF16),
            V((2, 16, 256), BF16),
            V((8, 128), F32),
            V((SPN, 8, 128), F32),
            V((6, ROWS, 1024), BF16),
            V((2, ROWS, 1024), BF16),
            V((4, ROWS, 1024), BF16),
            V((ROWS, D), F32),
            V((512, Q), BF16),
            V((2048, 512), BF16),
            V((4, 512, 512), BF16),
            V((2048, Q), BF16),
            V((2048, Q), BF16),
            V((2048, Q), BF16),
            V((2048, Q), BF16),
            V((128, D), BF16),
            V((128, HID), BF16),
            V((2, 256, Q), BF16),
            V((512, Q), F32),
            V((4, 128, 128), F32),
            pltpu.SemaphoreType.DMA((23,)),
            pltpu.SemaphoreType.DMA((4,)),
            pltpu.SemaphoreType.DMA((2,)),
            pltpu.SemaphoreType.DMA((12,)),
            pltpu.SemaphoreType.DMA((5,)),
            pltpu.SemaphoreType.DMA((5,)),
        ],
        compiler_params=pltpu.CompilerParams(
            collective_id=0, has_side_effects=True, vmem_limit_bytes=58 * 1024 * 1024
        ),
        name="layer",
    )(*operands)


def solution(mesh):
    placed = (
        P(("sp", "tp"), None),
        P("sp", "tp"),
        P("sp", "tp"),
        P("sp", "tp"),
        P("sp", "tp"),
        P(None, "tp"),
        P(None, "tp"),
        P("tp", None, None),
        P("tp", None, None),
        P("tp", None, None),
        P("tp", None, None),
        P("tp"),
        P("tp"),
        P("sp"),
        P("tp", None),
        P("tp", None),
        P(),
        P(("sp", "tp"), None),
        P(("sp", "tp")),
        P(("sp", "tp")),
        P(("sp", "tp"), None, None),
        P(("sp", "tp"), None, None),
        P(("sp", "tp"), None, None),
    )
    return jax.shard_map(
        shards, mesh=mesh, in_specs=placed, out_specs=P(("sp", "tp"), None), check_vma=False
    )
```

```python
import random

import jax
import jax.numpy as jnp
from jax import lax
from jax.experimental import pallas as pl
from jax.experimental.pallas import tpu as pltpu
from jax.sharding import PartitionSpec as P

EPSILON = 1e-06
GATE_SCALE = 8.0
F32 = jnp.float32
BF16 = jnp.bfloat16
MESH = pl.DeviceIdType.MESH
ROWS = 128
LEN = 512
CH = 512
D = 2048
Q = 512
HID = 1024
SPN = 32


def dot(a, b):
    return jnp.dot(a, b, preferred_element_type=F32)


def iota(shape, dim):
    return lax.broadcasted_iota(jnp.int32, shape, dim)


def one_minus_square(log, a):
    u = -2.0 * log
    series = u * (1.0 - u * (0.5 - u * (1.0 / 6 - u * (1.0 / 24 - u * (1.0 / 120)))))
    return jnp.where(u < 0.05, series, 1.0 - a * a)


def softplus_neg(d):
    y = jnp.exp(-jnp.abs(d))
    w = 1.0 + y
    near = w - 1.0
    log1p = jnp.where(near == 0.0, y, jnp.log(w) * (y / jnp.where(near == 0.0, 1.0, near)))
    return jnp.maximum(-d, 0.0) + log1p


def hops(step):
    return -sum(min(n, 4 - n) for n in (step[0], step[1], step[3]))


def class_steps(c, seed):
    steps = []
    for j in range(32):
        dc, dx, dy = j % 2, (j // 2) % 4, j // 8
        steps.append((j, ((c - dx - dy) % 4, dy, dc, dx)))
    steps = [s for s in steps if any(s[1])]
    random.Random(seed).shuffle(steps)
    return steps


SENDS = [class_steps(c, c + 1) for c in range(4)]
REPLIES = [class_steps(c, c + 77) for c in range(4)]


def kernel(
    stream_far,
    cia_far,
    cib_far,
    gia_far,
    gib_far,
    cwa_far,
    cwb_far,
    rga_far,
    iga_far,
    rgb_far,
    igb_far,
    da_far,
    db_far,
    inc_far,
    owa_far,
    owb_far,
    gain_far,
    ids_far,
    gp_far,
    pg_far,
    wg_far,
    wu_far,
    wd_far,
    out,
    stream,
    cia,
    cib,
    gia,
    gib,
    cwa,
    cwb,
    rga,
    iga,
    rgb,
    igb,
    da,
    db,
    inc,
    gain,
    ids,
    gp,
    pg,
    wg,
    wu,
    wd,
    ow,
    xs,
    wb,
    incb,
    a8,
    h8,
    gl,
    hid,
    halo,
    stat,
    carry_in,
    psend,
    rd2,
    prec,
    p0,
    nq,
    mp,
    gm,
    sendb,
    recvb,
    replyb,
    retb,
    xb,
    inner,
    yb,
    acc,
    keys,
    lsem,
    hsem,
    csem,
    psem,
    dsem,
    rsem,
):
    sp = lax.axis_index("sp")
    x = lax.axis_index("tp")
    z, y, core = sp // 8, (sp // 2) % 4, sp % 2

    xs_at = [lax.rem(x + n, 4) for n in range(4)]
    ys_at = [lax.rem(y + n, 4) * 2 for n in range(4)]
    zs_at = [lax.rem(z + n, 4) * 8 for n in range(4)]
    cores_at = [core, 1 - core]
    yc_at = [[ys_at[n] + cores_at[m] for m in range(2)] for n in range(4)]

    def peer(step, sign=1):
        dz, dy, dc, dx = (sign * n for n in step)
        return {"sp": zs_at[dz % 4] + yc_at[dy % 4][dc % 2], "tp": xs_at[dx % 4]}

    barrier = pltpu.get_barrier_semaphore()
    for step in sorted((step for steps in SENDS for _, step in steps), key=hops):
        pl.semaphore_signal(barrier, inc=1, device_id=peer(step), device_id_type=MESH)
    pairs = (
        (cia_far, cia),
        (cib_far, cib),
        (cwa_far, cwa),
        (cwb_far, cwb),
        (rga_far, rga),
        (iga_far, iga),
        (rgb_far, rgb),
        (igb_far, igb),
        (da_far, da),
        (db_far, db),
        (inc_far, inc),
        (ids_far, ids),
        (gp_far, gp),
        (pg_far, pg),
        (gia_far, gia),
        (gib_far, gib),
        (owa_far, ow.at[pl.ds(0, 256)]),
        (owb_far, ow.at[pl.ds(256, 256)]),
        (stream_far, stream),
        (gain_far, gain),
        (wg_far.at[0], wg),
        (wu_far.at[0], wu),
        (wd_far.at[0], wd),
    )
    copies = [pltpu.make_async_copy(src, dst, lsem.at[n]) for n, (src, dst) in enumerate(pairs)]
    for copy in copies:
        copy.start()
    early, middle_loads, loads = copies[:14], copies[14:16], copies[16:]

    for load in early:
        load.wait()

    for n, (a_ref, b_ref) in enumerate(((rga, rgb), (iga, igb))):
        for h in range(4):
            place = (iota((64, 256), 1) == iota((64, 256), 0) + 64 * h).astype(BF16)
            wb[n, 64 * h : 64 * h + 64, :] = dot(a_ref[h], place).astype(BF16)
        wb[2 + n] = jnp.zeros((256, 256), BF16)
        for h in range(2):
            wb[2 + n, 128 * h : 128 * h + 128, 128 * h : 128 * h + 128] = b_ref[h]

    for n in range(4):
        row = jnp.broadcast_to(inc[:, 128 * n : 128 * n + 128], (128, 128))
        incb[128 * n : 128 * n + 128, :] = row.T

    xs[0:8, :] = jnp.zeros((8, CH), F32)
    xs[8 : 8 + LEN, 0:256] = cia[...].astype(F32)
    xs[8 : 8 + LEN, 256:512] = cib[...].astype(F32)

    plus = softplus_neg(jnp.concatenate([da[...], db[...]], axis=1)) * GATE_SCALE

    def chunk(r0, size):
        jump = incb[pl.ds(r0, size), :]
        jump = jnp.concatenate([jump, jump], axis=1)
        for side, taps in enumerate((cwa, cwb)):
            lanes = slice(256 * side, 256 * side + 256)
            window = xs[pl.ds(r0, size + 8), lanes]
            tap = taps[...].astype(F32)
            total = tap[0:1] * pltpu.roll(window, 3, 0)[8:]
            total = total + tap[1:2] * pltpu.roll(window, 2, 0)[8:]
            total = total + tap[2:3] * pltpu.roll(window, 1, 0)[8:]
            total = total + tap[3:4] * window[8:]
            conv = total.astype(BF16)
            rec = jax.nn.sigmoid(dot(conv, wb[2 * side]))
            admit = 0.5 * jnp.tanh(0.5 * dot(conv, wb[2 * side + 1])) + 0.5
            log = jump - rec * plus[:, lanes]
            a = jnp.exp(log)
            gone = one_minus_square(log, a)
            root = gone * lax.rsqrt(jnp.maximum(gone, 1e-37))
            h = root * admit * conv.astype(F32)
            a3, h3 = a.reshape(-1, 8, 256), h.reshape(-1, 8, 256)
            at = iota((size // 8, 8, 256), 1)
            for s in (1, 2, 4):
                ok = at >= s
                ap = jnp.where(ok, pltpu.roll(a3, s, 1), 1.0)
                hp = jnp.where(ok, pltpu.roll(h3, s, 1), 0.0)
                h3 = h3 + a3 * hp
                a3 = a3 * ap
            a8[pl.ds(r0, size), lanes] = a3.reshape(size, 256)
            h8[pl.ds(r0, size), lanes] = h3.reshape(size, 256)

    def later_chunks(step, carry):
        chunk(pl.multiple_of((7 - step) * 64, 64), 64)
        return carry

    lax.fori_loop(0, 4, later_chunks, 0)
    pl.semaphore_wait(barrier, 127)
    nextsp = {"sp": (sp + 1) % SPN, "tp": x}
    halos = [
        pltpu.make_async_remote_copy(
            ref.at[pl.ds(LEN - 16, 16)],
            halo.at[n],
            hsem.at[n],
            hsem.at[2 + n],
            device_id=nextsp,
            device_id_type=MESH,
        )
        for n, ref in enumerate((cia, cib))
    ]
    for copy in halos:
        copy.start()

    lax.fori_loop(4, 8, later_chunks, 0)

    def slab(r0, prod, state):
        a, h = a8[pl.ds(r0, 8), :], h8[pl.ds(r0, 8), :]
        h = h + a * state
        a = a * prod
        a8[pl.ds(r0, 8), :] = a
        h8[pl.ds(r0, 8), :] = h
        return a[7:8], h[7:8]

    def link(step, carry):
        prod, state = carry
        for n in range(8):
            prod, state = slab(pl.multiple_of(step * 64, 64) + 8 * n, prod, state)
        return prod, state

    prod, state = jnp.ones((1, CH), F32), jnp.zeros((1, CH), F32)
    for n in range(1, 8):
        prod, state = slab(8 * n, prod, state)
    prod, state = lax.fori_loop(1, 8, link, (prod, state))

    for copy in halos:
        copy.wait()
    keep = jnp.where(sp > 0, 1.0, 0.0)
    xs[0:8, 0:256] = halo[0].astype(F32)[8:16] * keep
    xs[0:8, 256:512] = halo[1].astype(F32)[8:16] * keep
    chunk(0, 8)
    head_prod, head_state = a8[7:8, :], h8[7:8, :]
    state = state + prod * head_state
    prod = prod * head_prod

    for n in range(4):
        stat[n : n + 1, :] = prod[:, 128 * n : 128 * n + 128]
        stat[4 + n : 5 + n, :] = state[:, 128 * n : 128 * n + 128]

    for k in sorted(range(1, SPN), key=lambda k: -(min(k // 8, 4 - k // 8) + min(k // 2 % 4, 4 - k // 2 % 4))):
        pltpu.make_async_remote_copy(
            stat,
            carry_in.at[k],
            csem.at[0],
            csem.at[1],
            device_id={"sp": lax.rem(sp + k, SPN), "tp": x},
            device_id_type=MESH,
        ).start()
    told = carry_in.at[pl.ds(1, SPN - 1)]

    e0r = jnp.broadcast_to(ids[0:1, :].astype(F32), (128, 128))
    e1r = jnp.broadcast_to(ids[1:2, :].astype(F32), (128, 128))
    e0, e1 = e0r.T, e1r.T
    earlier = iota((128, 128), 0) < iota((128, 128), 1)
    for n, er in enumerate((e0r, e1r)):
        hits = jnp.where(earlier & (e0 == er), 1.0, 0.0) + jnp.where(earlier & (e1 == er), 1.0, 0.0)
        rank = jnp.sum(hits, axis=0, keepdims=True).astype(jnp.int32)
        e = er[0:1].astype(jnp.int32)
        ez, ey, ec, ex = e // 32, (e // 8) % 4, (e // 4) % 2, e % 4
        dz, dy, dc, dx = (ez - z + 4) % 4, (ey - y + 4) % 4, (ec - core + 2) % 2, (ex - x + 4) % 4
        key = (((dx + dy + dz) % 4) * 32 + dy * 8 + dx * 2 + dc) * 16 + rank
        keys[n] = jnp.broadcast_to(key.astype(F32), (128, 128))
    first = gp[...] * jax.nn.sigmoid(pg[...])
    second = gp[...] * jax.nn.sigmoid(-pg[...])
    keys[2] = jnp.broadcast_to(first, (128, 128)).T
    keys[3] = jnp.broadcast_to(second, (128, 128)).T

    def pack_matrix(step, carry):
        r0 = pl.multiple_of(step * 128, 128)
        rho = (iota((128, 128), 0) + r0).astype(F32)
        k0, k1 = keys[0], keys[1]
        for q in range(4):
            hit = (rho == k0 + 4.0 * q) | (rho == k1 + 4.0 * q)
            mp[pl.ds(r0, 128), 128 * q : 128 * q + 128] = jnp.where(hit, 1.0, 0.0).astype(BF16)
        return carry

    lax.fori_loop(0, 16, pack_matrix, 0)

    keys[0] = keys[0].T
    keys[1] = keys[1].T

    def pick_matrix(c, carry):
        k0, k1, w0, w1 = keys[0], keys[1], keys[2], keys[3]
        for lane in range(4):
            rho = (iota((128, 128), 1) + (c * 512 + 128 * lane)).astype(F32)
            cols = slice(128 * lane, 128 * lane + 128)
            for q in range(4):
                val = jnp.where(rho == k0 + 4.0 * q, w0, 0.0)
                val = val + jnp.where(rho == k1 + 4.0 * q, w1, 0.0)
                gm[c, 128 * q : 128 * q + 128, cols] = val.astype(BF16)
        return carry

    lax.fori_loop(0, 4, pick_matrix, 0)

    for load in middle_loads:
        load.wait()

    def gelus(step, carry):
        r0 = pl.multiple_of(step * 64, 64)
        gl[pl.ds(r0, 64), 0:256] = jax.nn.gelu(gia[pl.ds(r0, 64), :].astype(F32))
        gl[pl.ds(r0, 64), 256:512] = jax.nn.gelu(gib[pl.ds(r0, 64), :].astype(F32))
        return carry

    lax.fori_loop(0, 8, gelus, 0)

    pltpu.make_async_copy(told, told, csem.at[1]).wait()

    enter = jnp.zeros((4, 128), F32)
    for k in range(SPN - 1, 0, -1):
        enter = jnp.where(k <= sp, carry_in[k, 0:4] * enter + carry_in[k, 4:8], enter)
    enter = jnp.concatenate([enter[n : n + 1] for n in range(4)], axis=1)

    h8[0:8, :] = h8[0:8, :] + a8[0:8, :] * enter
    a8[0:8, :] = jnp.zeros((8, CH), F32)
    enter = head_state + head_prod * enter

    def hiddens(step, carry):
        r0 = pl.multiple_of(lax.rem(step + 2 * x + 4, 8) * 64, 64)
        states = h8[pl.ds(r0, 64), :] + a8[pl.ds(r0, 64), :] * enter
        hid[pl.ds(r0, 64), :] = (states * gl[pl.ds(r0, 64), :]).astype(BF16)
        return carry

    loads[0].wait()
    loads[1].wait()
    lax.fori_loop(0, 2, hiddens, 0)

    def rows_for(d):
        return hid[pl.ds(pl.multiple_of(((x + d) % 4) * 128, 128), 128), :]

    def project(d, half, extra=None):
        rows = rows_for(d)
        for n in range(2):
            at = 1024 * half + 512 * n
            part = dot(rows, ow[:, at : at + 512])
            if extra is not None:
                part = part + extra[:, 512 * n : 512 * n + 512].astype(F32)
            psend[2 * d + half - 2, :, 512 * n : 512 * n + 512] = part.astype(BF16)

    def push(d, half, dst, sem, dx):
        copy = pltpu.make_async_remote_copy(
            psend.at[2 * d + half - 2],
            dst,
            psem.at[2 * sem],
            psem.at[2 * sem + 1],
            device_id={"sp": sp, "tp": (x + dx) % 4},
            device_id_type=MESH,
        )
        copy.start()
        return copy

    project(2, 0)
    sums = [push(2, 0, rd2.at[0], 0, 1)]
    project(2, 1)
    sums.append(push(2, 1, rd2.at[1], 1, 3))
    lax.fori_loop(2, 8, hiddens, 0)
    project(1, 1)
    sums.append(push(1, 1, prec.at[1], 2, 1))
    project(3, 0)
    sums.append(push(3, 0, prec.at[2], 3, 3))
    own = rows_for(0)
    for n in range(4):
        p0[:, 512 * n : 512 * n + 512] = dot(own, ow[:, 512 * n : 512 * n + 512])
    sums[0].wait_recv()
    project(1, 0, rd2.at[0])
    sums.append(push(1, 0, prec.at[0], 4, 1))
    sums[1].wait_recv()
    project(3, 1, rd2.at[1])
    sums.append(push(3, 1, prec.at[3], 5, 3))
    loads[2].wait()
    loads[3].wait()
    for copy in sums[2:4]:
        copy.wait_recv()

    def gather(step, carry):
        rows = pl.ds(pl.multiple_of(step * 16, 16), 16)
        part = jnp.concatenate([prec[2, rows, :], prec[1, rows, :]], axis=1).astype(F32)
        p0[rows, :] = p0[rows, :] + part + stream[rows, :].astype(F32)
        return carry

    lax.fori_loop(0, 8, gather, 0)
    for copy in sums[4:]:
        copy.wait_recv()
    gains = gain[...].astype(F32)
    gains = jnp.concatenate([gains[n : n + 1] for n in range(16)], axis=1)

    def norms(step, carry):
        r0 = pl.multiple_of(step * 16, 16)
        rows = pl.ds(r0, 16)
        part = jnp.concatenate([prec[0, rows, :], prec[3, rows, :]], axis=1).astype(F32)
        middle = (p0[rows, :] + part).astype(BF16).astype(F32)
        scale = lax.rsqrt(jnp.mean(middle * middle, axis=-1, keepdims=True) + EPSILON)
        normed = (middle * scale * gains).astype(BF16)
        for q in range(4):
            acc[pl.ds(128 * q + r0, 16), :] = middle[:, 512 * q : 512 * q + 512]
            nq[pl.ds(128 * q + r0, 16), :] = normed[:, 512 * q : 512 * q + 512]
        return carry

    lax.fori_loop(0, 8, norms, 0, unroll=4)

    def send_class(c, src, dst, sem, sign):
        for n, steps in enumerate(SENDS if sign > 0 else REPLIES):

            @pl.when(c == n)
            def _(n=n, steps=steps):
                for j, step in steps:
                    tile = pl.ds(512 * n + 16 * j, 16)
                    pltpu.make_async_remote_copy(
                        src.at[tile],
                        dst.at[tile],
                        sem.at[0],
                        sem.at[1 + n],
                        device_id=peer(step, sign),
                        device_id_type=MESH,
                    ).start()

    def dispatch(c, carry):
        for n in range(4):
            r0 = pl.multiple_of(c * 512, 512) + 128 * n
            sendb[pl.ds(r0, 128), :] = dot(mp[pl.ds(r0, 128), :], nq[...]).astype(BF16)

        send_class(c, sendb, recvb, dsem, 1)
        return carry

    lax.fori_loop(0, 4, dispatch, 0)
    recvb[0:16, :] = sendb[0:16, :]

    for load in loads[4:]:
        load.wait()

    def wait_class(buf, sem, c):
        if isinstance(c, int):
            part = buf.at[pl.ds(c * 512, 512)]
            pltpu.make_async_copy(part, part, sem.at[1 + c]).wait()
            return

        @pl.when(c == 0)
        def _():
            part = buf.at[pl.ds(16, 496)]
            pltpu.make_async_copy(part, part, sem.at[1]).wait()

        @pl.when(c > 0)
        def _():
            part = buf.at[pl.ds(pl.multiple_of(c * 512, 512), 512)]
            pltpu.make_async_copy(part, part, sem.at[1 + c]).wait()

    def experts(c, carry):
        wait_class(recvb, dsem, c)
        ra, rb = iota((256, 256), 0), iota((256, 256), 1)
        sort = (rb == ((ra % 64) // 4) * 16 + (ra // 64) * 4 + ra % 4).astype(F32).astype(BF16)
        unsort = (ra == ((rb % 64) // 4) * 16 + (rb // 64) * 4 + rb % 4).astype(F32).astype(BF16)
        for half in range(2):
            r0 = pl.multiple_of(c * 512, 512) + 256 * half
            got = dot(sort, recvb[pl.ds(r0, 256), :]).astype(BF16)
            for q in range(4):
                xb[64 * half : 64 * half + 64, 512 * q : 512 * q + 512] = got[64 * q : 64 * q + 64]
        for n in range(4):
            cols = slice(256 * n, 256 * n + 256)
            gate = dot(xb[...], wg[:, cols])
            up = dot(xb[...], wu[:, cols])
            inner[:, cols] = (jax.nn.silu(gate) * up).astype(BF16)
        for q in range(4):
            down = dot(inner[...], wd[:, 512 * q : 512 * q + 512]).astype(BF16)
            for half in range(2):
                yb[half, 64 * q : 64 * q + 64, :] = down[64 * half : 64 * half + 64]
        for half in range(2):
            r0 = pl.multiple_of(c * 512, 512) + 256 * half
            replyb[pl.ds(r0, 256), :] = dot(unsort, yb[half]).astype(BF16)

        send_class(c, replyb, retb, rsem, -1)
        return carry

    lax.fori_loop(0, 4, experts, 0)
    retb[0:16, :] = replyb[0:16, :]

    def combine(c, carry):
        wait_class(retb, rsem, c)
        got = pl.ds(pl.multiple_of(c * 512, 512), 512)
        for n in range(4):
            rows = slice(128 * n, 128 * n + 128)
            acc[rows, :] = acc[rows, :] + dot(gm[c, rows, :], retb[got, :])
        return carry

    lax.fori_loop(0, 3, combine, 0)
    wait_class(retb, rsem, 3)
    for q in range(4):
        rows = slice(128 * q, 128 * q + 128)
        total = acc[rows, :] + dot(gm[3, rows, :], retb[1536:2048, :])
        out[:, 512 * q : 512 * q + 512] = total.astype(BF16)

    pltpu.make_async_copy(told, told, csem.at[0]).wait()
    for copy in sums:
        copy.wait_send()
    for buf, sem in ((sendb, dsem), (replyb, rsem)):
        part = buf.at[pl.ds(16, 2032)]
        pltpu.make_async_copy(part, part, sem.at[0]).wait()


def shards(*args):
    (
        stream,
        cia,
        cib,
        gia,
        gib,
        cwa,
        cwb,
        rga,
        iga,
        rgb,
        igb,
        da,
        db,
        inc,
        owa,
        owb,
        gain,
        ids,
        gp,
        pg,
        wg,
        wu,
        wd,
    ) = args
    row = lambda a: a.reshape(1, -1)
    operands = (
        stream,
        cia,
        cib,
        gia,
        gib,
        cwa,
        cwb,
        rga,
        iga,
        rgb,
        igb,
        row(da),
        row(db),
        row(inc),
        owa,
        owb,
        gain.reshape(16, 128),
        ids.T,
        row(gp),
        row(pg),
        wg,
        wu,
        wd,
    )
    vmem = pl.BlockSpec(memory_space=pltpu.VMEM)
    far = pl.BlockSpec(memory_space=pl.ANY)
    V = pltpu.VMEM
    near = [V(a.shape, a.dtype) for n, a in enumerate(operands[:20]) if n not in (14, 15)]
    return pl.pallas_call(
        kernel,
        out_shape=pltpu.VMEM((ROWS, D), BF16),
        in_specs=[far] * len(operands),
        out_specs=vmem,
        scratch_shapes=near
        + [
            V((D, HID), BF16),
            V((D, HID), BF16),
            V((HID, D), BF16),
            V((CH, D), BF16),
            V((LEN + 8, CH), F32),
            V((4, 256, 256), BF16),
            V((LEN, 128), F32),
            V((LEN, CH), F32),
            V((LEN, CH), F32),
            V((LEN, CH), F32),
            V((LEN, CH), BF16),
            V((2, 16, 256), BF16),
            V((8, 128), F32),
            V((SPN, 8, 128), F32),
            V((6, ROWS, 1024), BF16),
            V((2, ROWS, 1024), BF16),
            V((4, ROWS, 1024), BF16),
            V((ROWS, D), F32),
            V((512, Q), BF16),
            V((2048, 512), BF16),
            V((4, 512, 512), BF16),
            V((2048, Q), BF16),
            V((2048, Q), BF16),
            V((2048, Q), BF16),
            V((2048, Q), BF16),
            V((128, D), BF16),
            V((128, HID), BF16),
            V((2, 256, Q), BF16),
            V((512, Q), F32),
            V((4, 128, 128), F32),
            pltpu.SemaphoreType.DMA((23,)),
            pltpu.SemaphoreType.DMA((4,)),
            pltpu.SemaphoreType.DMA((2,)),
            pltpu.SemaphoreType.DMA((12,)),
            pltpu.SemaphoreType.DMA((5,)),
            pltpu.SemaphoreType.DMA((5,)),
        ],
        compiler_params=pltpu.CompilerParams(
            collective_id=0, has_side_effects=True, vmem_limit_bytes=58 * 1024 * 1024
        ),
        name="layer",
    )(*operands)


def solution(mesh):
    placed = (
        P(("sp", "tp"), None),
        P("sp", "tp"),
        P("sp", "tp"),
        P("sp", "tp"),
        P("sp", "tp"),
        P(None, "tp"),
        P(None, "tp"),
        P("tp", None, None),
        P("tp", None, None),
        P("tp", None, None),
        P("tp", None, None),
        P("tp"),
        P("tp"),
        P("sp"),
        P("tp", None),
        P("tp", None),
        P(),
        P(("sp", "tp"), None),
        P(("sp", "tp")),
        P(("sp", "tp")),
        P(("sp", "tp"), None, None),
        P(("sp", "tp"), None, None),
        P(("sp", "tp"), None, None),
    )
    return jax.shard_map(
        shards, mesh=mesh, in_specs=placed, out_specs=P(("sp", "tp"), None), check_vma=False
    )
```
